32 devices in a mesh: ep: 8 (over z, y), tp: 4 (over x, core).
Axes of the slice: x: 2, y: 2, z: 4, core: 2. Of those that a mesh axis runs over, the one named last changes fastest.
Arguments:
- tokens: bfloat16 [1024, 2048], P('ep'), may hold values from -6 to 6
- cotangent: bfloat16 [1024, 2048], P('ep'), may hold values from -2 to 2
- route_weights: float32 [1024, 2], P('ep'), may hold values from 0.25 to 2.5
- routes: int32 [1024, 2], P('ep'), may hold values from 0 to 7, all different within a row; in each aligned block of 128 rows (0 to 127, 128 to 255, ...) at most 64 rows name the same one
- gate_proj: bfloat16 [8, 2048, 512], P('ep', None, 'tp'), may hold values from -0.125 to 0.125
- up_proj: bfloat16 [8, 2048, 512], P('ep', None, 'tp'), may hold values from -0.125 to 0.125
- down_proj: bfloat16 [8, 512, 2048], P('ep', 'tp'), may hold values from -0.25 to 0.25
- shared_down: bfloat16 [2048, 512], P(None, 'tp'), may hold values from -0.25 to 0.25
- shared_hidden: bfloat16 [1024, 512], P('ep', 'tp'), may hold values from -0.29882812 to 0.29882812
Outputs:
- tokens_grad: bfloat16 [1024, 2048], P('ep', 'tp')
- weights_grad: float32 [1024, 2], P('ep')
- gate_proj_grad: bfloat16 [8, 2048, 512], P('ep', None, 'tp')
- up_proj_grad: bfloat16 [8, 2048, 512], P('ep', None, 'tp')
- down_proj_grad: bfloat16 [8, 512, 2048], P('ep', 'tp')
- hidden_grad: bfloat16 [1024, 512], P('ep', 'tp')
- shared_grad: float32 [2048, 512], P('ep', 'tp')
The draws below stay inside these ranges and needn't reach their ends.
Inputs may be any that keep to these rules, and one draw needn't show every extreme that they name: `routes`: in each aligned block of 128 rows no expert is named more than 64 times, a bound that some block reaches; the 2 experts of a row differ.
All inputs are finite; a program needn't handle non-finite values.
Results may differ from the reference program's by a relative error of at most 0.012.
Values may be sent and summed in bfloat16 or wider, within the bound.
A program may use at most 64 MiB of HBM per device.

```python
import math
import jax
import jax.numpy as jnp
import numpy as np
from jax import lax

D = 2048
FF = 512
D_SHARED = 512
TOP = 2
TOK_DEV = 128
EXPERTS = 8
TOKENS = 1024
CAP = 64
N_EP = 8
N_TP = 4


def raised(values, stream_key, source, target, parts, factor):
    def block_of(position):
        return (jnp.arange(values.shape[position]) // (values.shape[position] // parts)).reshape((-1,) + (1,) * (values.ndim - 1 - position))

    near = jax.random.permutation(stream_key, parts)[block_of(target)]
    other_side = (block_of(target) + parts // 2) % parts
    return jnp.where((block_of(source) == near) | (block_of(source) == other_side), factor * values, values)


def block_levels(stream_key, extent, shards, low, top_value):
    factor_of, own = 1.0, jax.random.fold_in(stream_key, 6)
    for axis_at, shards_of in shards:
        draws = jnp.exp(jax.random.uniform(jax.random.fold_in(own, axis_at), (shards_of,), jnp.float32, low / len(shards), top_value / len(shards)))
        factor_of = factor_of * jnp.repeat(draws, extent[axis_at] // shards_of).reshape([-1 if axis == axis_at else 1 for axis in range(len(extent))])
    return factor_of


def assign_block(rng, own, number, rows, count, top, limit, lean):
    sequence = jax.random.permutation(rng, count)
    heavy_load, common = load_shares(count, rows * top, limit, lean, True), load_shares(count, rows * top, limit, lean, False)
    places = jnp.arange(count)

    def named(sizes, turn):
        used = int((sizes > 0).sum())
        fixed = max(1, used // 4)
        passed = fixed + (places - fixed + turn * (used - fixed)) % max(1, count - fixed)
        return jnp.zeros((count,), jnp.int32).at[sequence[jnp.where(places < fixed, places, passed)]].set(jnp.asarray(sizes, jnp.int32))

    sizes = jnp.where(number % 4 == 0, named(heavy_load, number // 4), named(common, number - number // 4 - 1))
    mixed = jax.random.permutation(jax.random.fold_in(own, 3), count)
    donor, sink = mixed[0:count // 2 * 2:2], mixed[1:count // 2 * 2:2]
    margin = jnp.minimum(sizes[donor] - 1, limit - sizes[sink]) // 2
    margin = jnp.where((donor == sequence[0]) | (sink == sequence[0]) | (sizes[sink] == 0), 0, jnp.maximum(margin, 0))
    passed = jax.random.randint(jax.random.fold_in(own, 4), (count // 2,), 0, 1 << 20) % (margin + 1)
    sizes = sizes.at[donor].add(-passed).at[sink].add(passed)
    items = jnp.searchsorted(jnp.cumsum(sizes), jnp.arange(rows * top), side="right").astype(jnp.int32)
    grid = items.reshape(top, rows).T
    grid = grid[jax.random.permutation(jax.random.fold_in(own, 1), rows)]
    turn = jax.random.randint(jax.random.fold_in(own, 2), (rows, 1), 0, top)
    return jnp.take_along_axis(grid, (jnp.arange(top)[None, :] + turn) % top, axis=1)


def load_shares(number_of, total, limit, lean, full):
    loads = [(1 << 20) // math.isqrt(rank ** lean) + 1 for rank in range(1, number_of + 1)]
    largest = limit if full else min(limit, max(-(-total // number_of), total * loads[0] // sum(loads)))
    least = 1 if total - largest >= number_of - 1 else 0
    counts, spare = [largest] + [least] * (number_of - 1), total - largest - least * (number_of - 1)
    while spare > 0:
        free = [i for i in range(1, number_of) if counts[i] < largest] or [i for i in range(1, number_of) if counts[i] < limit]
        mass, budget = sum([loads[i] for i in free]), spare
        for i in free:
            extra = min(limit - counts[i], max(1, budget * loads[i] // mass), spare)
            counts[i] = counts[i] + extra
            spare = spare - extra
    return np.array(counts)


def centred(own_key, shape, spread, limit, shards=(), kind=jnp.bfloat16):
    result = spread * jax.random.normal(own_key, shape, jnp.float32)
    if shards:
        result = result * block_levels(own_key, shape, shards, -0.22, 0.18)
    return jnp.clip(result, -limit, limit).astype(kind)


def noise_with(rng, extent, scale, most, split, heavy, kind=jnp.bfloat16):
    drawn = scale * jax.random.normal(rng, extent, jnp.float32)
    if split:
        drawn = drawn * block_levels(rng, extent, split, -0.22, 0.18)
    return jnp.clip(raised(drawn, jax.random.fold_in(rng, 3), *heavy), -most, most).astype(kind)


def setup_inputs(seed: int = 0) -> dict:
    seeds = jax.random.split(jax.random.key(seed), 10)
    tokens = centred(seeds[0], (TOKENS, D), 1.0, 6.0, ((0, 8),))
    cotangent = noise_with(seeds[1], (TOKENS, D), 0.25, 2.0, ((0, 8),), (0, 1, 8, 2.0))
    route_weights = jnp.clip(jnp.exp(math.log(2.5) - 2.3025851 * jax.random.uniform(seeds[2], (TOKENS, TOP), jnp.float32) ** block_levels(seeds[2], (TOKENS, TOP), ((0, 8),), -0.2, 0.2)), 0.25, 2.5)
    routes_keys = jax.random.split(jax.random.fold_in(seeds[3], 1), TOKENS // TOK_DEV)
    routes_turns = jax.random.permutation(jax.random.fold_in(seeds[3], 3), TOKENS // TOK_DEV)
    routes = jax.vmap(lambda own, number: assign_block(jax.random.fold_in(seeds[3], 2), own, number, TOK_DEV, EXPERTS, TOP, CAP, 2))(routes_keys, routes_turns).reshape((TOKENS, TOP))
    gate_proj = centred(seeds[4], (EXPERTS, D, FF), D ** -0.5, 0.125, ((0, 8), (2, 4)))
    up_proj = centred(seeds[5], (EXPERTS, D, FF), D ** -0.5, 0.125, ((0, 8), (2, 4)))
    down_proj = centred(seeds[6], (EXPERTS, FF, D), FF ** -0.5, 0.25, ((0, 8), (1, 4)))
    shared_down = centred(seeds[7], (D, D_SHARED), D_SHARED ** -0.5, 0.25, ((1, 4),))
    shared_hidden = centred(seeds[8], (TOKENS, D_SHARED), 0.05, 0.29882812, ((0, 8), (1, 4)))
    return {"tokens": tokens, "cotangent": cotangent, "route_weights": route_weights, "routes": routes, "gate_proj": gate_proj, "up_proj": up_proj, "down_proj": down_proj, "shared_down": shared_down, "shared_hidden": shared_hidden}


def slot_index(routes):
    blocks = routes.reshape(N_EP, TOK_DEV * TOP)
    one_hot = (blocks[:, :, None] == jnp.arange(EXPERTS, dtype=jnp.int32)[None, None, :]).astype(jnp.int32)
    earlier = jnp.cumsum(one_hot, axis=1) - one_hot
    rank_in = jnp.sum(earlier * one_hot, axis=2)
    source = jnp.arange(N_EP, dtype=jnp.int32)[:, None]
    return ((blocks * N_EP + source) * CAP + rank_in).astype(jnp.int32)


def one_expert(inputs):
    in_rows, in_grads, in_weights, w_gate, w_up, w_down = inputs
    gate = jnp.dot(in_rows, w_gate, preferred_element_type=jnp.float32)
    upper = jnp.dot(in_rows, w_up, preferred_element_type=jnp.float32)
    active = jax.nn.silu(gate)
    hidden = (active * upper).astype(jnp.bfloat16)
    backed = jnp.dot(in_grads, w_down.T, preferred_element_type=jnp.float32)
    gate_grad = jnp.sum(hidden.astype(jnp.float32) * backed, axis=1).astype(jnp.bfloat16)
    weight_col = in_weights.astype(jnp.float32)[:, None]
    d_hidden = weight_col * backed
    sigma = jax.nn.sigmoid(gate)
    d_gate = (d_hidden * upper * sigma * (1.0 + gate * (1.0 - sigma))).astype(jnp.bfloat16)
    d_up = (d_hidden * active).astype(jnp.bfloat16)
    scaled = (weight_col * in_grads.astype(jnp.float32)).astype(jnp.bfloat16)
    down_grad = jnp.dot(hidden.T, scaled, preferred_element_type=jnp.float32).astype(jnp.bfloat16)
    gate_wgrad = jnp.dot(in_rows.T, d_gate, preferred_element_type=jnp.float32).astype(jnp.bfloat16)
    up_wgrad = jnp.dot(in_rows.T, d_up, preferred_element_type=jnp.float32).astype(jnp.bfloat16)
    block_units = FF // N_TP
    slot_count = in_rows.shape[0]
    dg_blocks = d_gate.astype(jnp.float32).reshape(slot_count, N_TP, block_units)
    du_blocks = d_up.astype(jnp.float32).reshape(slot_count, N_TP, block_units)
    wg_blocks = w_gate.astype(jnp.float32).reshape(D, N_TP, block_units)
    wu_blocks = w_up.astype(jnp.float32).reshape(D, N_TP, block_units)
    partial_value = jnp.einsum("rtf,dtf->trd", dg_blocks, wg_blocks) + jnp.einsum("rtf,dtf->trd", du_blocks, wu_blocks)
    partial_value = lax.optimization_barrier(partial_value.astype(jnp.bfloat16))
    input_grad = jnp.sum(partial_value.astype(jnp.float32), axis=0).astype(jnp.bfloat16)
    return input_grad, gate_grad, gate_wgrad, up_wgrad, down_grad


def reference(tokens, cotangent, route_weights, routes, gate_proj, up_proj, down_proj, shared_down, shared_hidden):
    slot_ids = slot_index(routes).reshape(-1)
    owner_ids = jnp.arange(TOKENS * TOP, dtype=jnp.int32) // TOP
    total_slots = EXPERTS * N_EP * CAP
    per_expert = N_EP * CAP
    row_buf = jnp.zeros((total_slots, D), jnp.bfloat16).at[slot_ids].set(tokens[owner_ids])
    grad_buf = jnp.zeros((total_slots, D), jnp.bfloat16).at[slot_ids].set(cotangent[owner_ids])
    weight_buf = jnp.zeros((total_slots,), jnp.bfloat16).at[slot_ids].set(route_weights.reshape(-1).astype(jnp.bfloat16))
    results = lax.map(one_expert, (row_buf.reshape(EXPERTS, per_expert, D), grad_buf.reshape(EXPERTS, per_expert, D),
                                   weight_buf.reshape(EXPERTS, per_expert), gate_proj, up_proj, down_proj))
    input_grad, gate_grad, gate_wgrad, up_wgrad, down_grad = results
    picked = input_grad.reshape(total_slots, D)[slot_ids].reshape(TOKENS, TOP, D)
    tokens_grad = jnp.sum(picked.astype(jnp.float32), axis=1).astype(jnp.bfloat16)
    weights_grad = gate_grad.reshape(total_slots)[slot_ids].astype(jnp.float32).reshape(TOKENS, TOP)
    hidden_grad = jnp.dot(cotangent, shared_down, preferred_element_type=jnp.float32).astype(jnp.bfloat16)
    shared_grad = jnp.dot(cotangent.T, shared_hidden, preferred_element_type=jnp.float32)
    return tokens_grad, weights_grad, gate_wgrad, up_wgrad, down_grad, hidden_grad, shared_grad
```

```python
import functools

import jax
import jax.numpy as jnp
from jax import lax
from jax.experimental import pallas as pl
from jax.experimental.pallas import tpu as pltpu
from jax.sharding import PartitionSpec as P

MESH = pl.DeviceIdType.MESH
BF = jnp.bfloat16
F32 = jnp.float32
S_ZO, S_ZR, S_TO, S_TR, S_Y, S_YW, S_FX, S_C0, S_C = range(9)
S_RC, S_RX, S_GC, S_GX, S_RE, S_RG, S_SHARE, S_PAIR, SENDS = range(9, 18)
COUNTS = {
    "ZF": 8,
    "ZT": 4,
    "Y0": 1,
    "YF": 6,
    "YW": 4,
    "FX": 6,
    "CORE": 4,
    "RC": 5,
    "RX": 5,
    "GC": 5,
    "GX": 5,
    "RE": 1,
    "RG": 1,
    "SHARE": 1,
    "PAIR": 1,
}
FIRST = {kind: sum(list(COUNTS.values())[:i]) for i, kind in enumerate(COUNTS)}
ARRIVALS = sum(COUNTS.values())


def dot_f32(a, b, dims):
    return lax.dot_general(a, b, (dims, ((), ())), preferred_element_type=F32)


def kernel(
    n,
    cap,
    tok_ref,
    cot_ref,
    rw_ref,
    rt_ref,
    wg_ref,
    wu_ref,
    wd_ref,
    sd_ref,
    sh_ref,
    otok_ref,
    ow_ref,
    og_ref,
    ou_ref,
    od_ref,
    ohid_ref,
    osh_ref,
    xg,
    rwv,
    rtv,
    shv,
    zbuf,
    tiles,
    cperm,
    perm,
    ysend,
    wysend,
    wrecv,
    abuf,
    wgu,
    wdv,
    sdv,
    gradv,
    hw,
    dgu,
    part,
    crecv,
    keep,
    xsend,
    xrecv,
    rsend,
    ret,
    gpart,
    gcore,
    gtwo,
    gx,
    gsend,
    gret,
    ssend,
    spair,
    ssum,
    srecv,
    send_sem,
    recv_sem,
    load_sem,
    store_sem,
):
    me = lax.axis_index("ep")
    tp = lax.axis_index("tp")
    tok_rows, feat = tok_ref.shape
    top = rt_ref.shape[0]
    quarter = feat // 4
    units = wg_ref.shape[1]
    planes = n // 2
    both_rows = 2 * cap
    y = lax.rem(me, 2)
    z = me // 2
    core_of = lax.rem(tp, 2)
    half_of = tp // 2
    tp_c = half_of * 2 + (1 - core_of)
    tp_x = (1 - half_of) * 2 + core_of
    tp_xc = (1 - half_of) * 2 + (1 - core_of)
    me_y = jnp.bitwise_xor(me, 1)
    inner = (z > 0) & (z < planes - 1)
    outer = (z == 0) | (z == planes - 1)
    source = [
        z,
        jnp.where(z == 0, 1, z - 1),
        jnp.where(z == 0, 2, jnp.where(z == planes - 1, planes - 2, z + 1)),
        jnp.where(z < planes // 2, planes - 1, 0),
    ]
    source[2] = jnp.where(z == planes - 1, planes - 3, source[2])

    def copy(out, kind, at, src_ref, dst_ref, ep_to, tp_to):
        return pltpu.make_async_remote_copy(
            src_ref=src_ref,
            dst_ref=dst_ref,
            send_sem=send_sem.at[out],
            recv_sem=recv_sem.at[FIRST[kind] + at],
            device_id=(ep_to, tp_to),
            device_id_type=MESH,
        )

    def landed(kind, at, whole_ref):
        copy(0, kind, at, whole_ref, whole_ref, me_y, tp).wait_recv()

    def left(out, whole_ref):
        copy(out, "ZT", 0, whole_ref, whole_ref, me_y, tp).wait_send()

    def rows(block_y):
        return pl.ds(pl.multiple_of(block_y * cap, cap), cap)

    def columns(block):
        return pl.ds(pl.multiple_of(block * quarter, quarter), quarter)

    barrier = pltpu.get_barrier_semaphore()
    for to in ((me_y, tp), (me, tp_c), (me, tp_x)):
        pl.semaphore_signal(barrier, inc=1, device_id=to, device_id_type=MESH)

    @pl.when(z > 0)
    def _():
        pl.semaphore_signal(barrier, inc=1, device_id=(me - 2, tp), device_id_type=MESH)

    @pl.when(z < planes - 1)
    def _():
        pl.semaphore_signal(barrier, inc=1, device_id=(me + 2, tp), device_id_type=MESH)

    loads = [
        pltpu.make_async_copy(src, dst, load_sem.at[i])
        for i, (src, dst) in enumerate(
            (
                (rt_ref, rtv),
                (rw_ref, rwv),
                (tok_ref, xg.at[0]),
                (cot_ref, xg.at[1]),
                (wg_ref, wgu.at[:, pl.ds(0, units)]),
                (wu_ref, wgu.at[:, pl.ds(units, units)]),
                (wd_ref, wdv),
                (sd_ref, sdv),
                (sh_ref, shv),
            )
        )
    ]
    for load in loads:
        load.start()

    before = jnp.where(
        lax.broadcasted_iota(jnp.int32, (tok_rows, tok_rows), 0)
        < lax.broadcasted_iota(jnp.int32, (tok_rows, tok_rows), 1),
        1.0,
        0.0,
    ).astype(BF)
    slot = lax.broadcasted_iota(jnp.int32, (cap, tok_rows), 0).astype(F32)
    two = jnp.where(
        lax.broadcasted_iota(jnp.int32, (8, tok_rows), 0) == 0,
        me.astype(F32),
        me_y.astype(F32),
    )
    at_zero = y == 0

    def place(values):
        low = jnp.where(at_zero, values, 0.0)
        return jnp.concatenate([low, values - low], axis=1)

    def read_tile(i):
        s = source[i]
        named = jnp.zeros((8, tok_rows), F32)
        weight = jnp.zeros((8, tok_rows), F32)
        for k in range(top):
            hit = tiles[s, k : k + 1, :] == two
            named = named + jnp.where(hit, 1.0, 0.0)
            weight = weight + jnp.where(hit, tiles[s, top + k : top + k + 1, :], 0.0)
        rank = dot_f32(named.astype(BF), before, ((1,), (0,)))
        picks = jnp.concatenate(
            [
                jnp.where(slot == rank[j : j + 1, :], named[j : j + 1, :], 0.0).astype(BF)
                for j in range(2)
            ],
            axis=0,
        )
        cperm[i] = picks
        slotted = dot_f32(weight.astype(BF), picks, ((1,), (1,)))
        wrecv[2 * s + y] = jnp.broadcast_to(place(slotted[0:1, 0:cap]), (8, both_rows))
        wysend[i] = jnp.broadcast_to(place(slotted[1:2, cap:both_rows]), (8, both_rows))
        copy(S_YW, "YW", i, wysend.at[i], wrecv.at[2 * s + y], me_y, tp).start()

    def yw_in(i):
        at = 2 * source[i] + (1 - y)
        return copy(S_YW, "YW", i, wrecv.at[at], wrecv.at[at], me_y, tp)

    def yf(i, p, block):
        at = "Y0" if i == 0 else "YF"
        src = ysend.at[planes if block is tp_x else i, p]
        dst = abuf.at[source[i], block, p, rows(y)]
        return copy(S_Y, at, 0 if i == 0 else 2 * (i - 1) + p, src, dst, me_y, tp)

    def z_own(up, p):
        to = me + 2 if up else me - 2
        return copy(S_ZO, "ZF", 2 * z + p, xg.at[p, :, columns(tp)], zbuf.at[z, p], to, tp)

    def zt_own(up):
        to = me + 2 if up else me - 2
        return copy(S_TO, "ZT", z, tiles.at[z], tiles.at[z], to, tp)

    def z_relay(i, p):
        s = source[i]
        to = jnp.where(s < z, me + 2, me - 2)
        return copy(S_ZR, "ZF", 2 * s + p, zbuf.at[s, p], zbuf.at[s, p], to, tp)

    def zt_relay(i):
        s = source[i]
        to = jnp.where(s < z, me + 2, me - 2)
        return copy(S_TR, "ZT", s, tiles.at[s], tiles.at[s], to, tp)

    def fx(i, j, p):
        block_y = y if j == 0 else 1 - y
        at = abuf.at[source[i], tp, p, rows(block_y)]
        return copy(S_FX, "FX", 2 * (i - 1) + p, at, at, me, tp_x)

    def to_core(i, p, block):
        at = abuf.at[source[i], block, p]
        if i == 0:
            at = abuf.at[source[i], block, p, rows(1 - y)]
        return copy(S_C0 if i == 0 else S_C, "CORE", i, at, at, me, tp_c)

    def pair(q):
        return copy(S_PAIR, "PAIR", 0, ssend.at[1 - y, q], spair.at[q], me_y, tp)

    def share(d):
        to = jnp.bitwise_xor(z, d)
        return copy(S_SHARE, "SHARE", 0, ssum.at[to], srecv.at[z], 2 * to + y, tp)

    def piece(i):
        if i == 0:
            return z, rows(y), cap
        if i == 1:
            return z, rows(1 - y), cap
        return source[i - 1], pl.ds(0, both_rows), both_rows

    def rc(i):
        s, at, _ = piece(i)
        return copy(S_RC, "RC", i, part.at[s, 1 - core_of, :, at], crecv.at[s, :, at], me, tp_c)

    def rx(i):
        s, at, _ = piece(i)
        return copy(S_RX, "RX", i, xsend.at[s, at], xrecv.at[s, at], me, tp_x)

    def gc(i):
        return copy(S_GC, "GC", i, gpart.at[i], gcore.at[i], me, tp_c)

    def gxc(i):
        return copy(S_GX, "GX", i, gtwo.at[i], gx.at[i], me, tp_x)

    def back(i, j):
        s = source[i]
        block_y = y if j == 0 else 1 - y
        return copy(
            S_RE, "RE", 0, rsend.at[s, rows(block_y)], ret.at[me], 2 * s + block_y, tp
        )

    def back_g(i, j):
        to = 2 * source[i] + (y if j == 0 else 1 - y)
        return copy(S_RG, "RG", 0, gsend.at[i + 1], gret.at[me], to, tp)

    def take(i, p, gate=None):
        def run():
            landed("ZF", 2 * source[i] + p, zbuf.at[source[i], p])

            @pl.when(inner)
            def _():
                z_relay(i, p).start()

        if gate is None:
            run()
        else:
            pl.when(gate)(run)

    def spread(i, p):
        moved = dot_f32(cperm[i], zbuf[source[i], p], ((1,), (0,))).astype(BF)
        abuf[source[i], tp, p, rows(y)] = moved[0:cap]
        ysend[i, p] = moved[cap:both_rows]
        yf(i, p, tp).start()
        fx(i, 0, p).start()

    def crossed(i):
        for p in range(2):
            landed("YF", 2 * (i - 1) + p, abuf.at[source[i], tp, p, rows(1 - y)])
            fx(i, 1, p).start()
            to_core(i, p, tp).start()

    def ready(i):
        yw_in(i).wait_recv()
        if i == 0:
            landed("CORE", 0, abuf.at[z, 0:2, :, rows(1 - y)])
        else:
            landed("CORE", i, abuf.at[source[i], 0:2])

    def joined(i, p):
        landed("FX", 2 * (i - 1) + p, abuf.at[source[i], tp_x, p])
        to_core(i, p, tp_x).start()

    def compute(i):
        s, at, m = piece(i)
        both = jnp.zeros((m, 2 * units), F32)
        backed = jnp.zeros((m, units), F32)
        for b in range(4):
            cols = slice(b * quarter, (b + 1) * quarter)
            both = both + dot_f32(abuf[s, b, 0, at], wgu[cols, :], ((1,), (0,)))
            backed = backed + dot_f32(abuf[s, b, 1, at], wdv[:, cols], ((1,), (1,)))
        gate = both[:, 0:units]
        upper = both[:, units : 2 * units]
        sigma = jax.nn.sigmoid(gate)
        active = gate * sigma
        hidden = (active * upper).astype(BF).astype(F32)
        if i == 0:
            wrow, first = wrecv[me, 0:1, :], y * cap
        elif i == 1:
            wrow, first = wrecv[me_y, 0:1, :], (1 - y) * cap
        else:
            wrow, first = wrecv[2 * s, 0:1, :] + wrecv[2 * s + 1, 0:1, :], 0
        eye = (
            lax.broadcasted_iota(jnp.int32, (m, both_rows), 0) + first
            == lax.broadcasted_iota(jnp.int32, (m, both_rows), 1)
        )
        wcol = jnp.sum(jnp.where(eye, wrow, 0.0), axis=1, keepdims=True)
        d_hidden = wcol * backed
        hw[s, at] = (wcol * hidden).astype(BF)
        d_both = jnp.concatenate(
            [
                (d_hidden * upper * sigma * (1.0 + gate * (1.0 - sigma))).astype(BF),
                (d_hidden * active).astype(BF),
            ],
            axis=1,
        )
        dgu[s, at] = d_both
        for b in range(4):
            cols = slice(b * quarter, (b + 1) * quarter)
            part[s, b % 2, b // 2, at] = dot_f32(d_both, wgu[cols, :], ((1,), (1,))).astype(BF)
        rc(i).start()
        sums = lax.dot_general(
            jnp.ones((8, units), F32),
            hidden * backed,
            (((1,), (1,)), ((), ())),
            precision=lax.Precision.HIGHEST,
            preferred_element_type=F32,
        )
        if i == 0:
            sums = place(sums)
        elif i == 1:
            low = jnp.where(at_zero, 0.0, sums)
            sums = jnp.concatenate([low, sums - low], axis=1)
        gpart[i] = sums
        gc(i).start()

    def core_sum(i):
        s, at, _ = piece(i)
        rc(i).wait_recv()
        xsend[s, at] = (
            part[s, core_of, 1 - half_of, at].astype(F32) + crecv[s, 1 - half_of, at].astype(F32)
        ).astype(BF)
        rx(i).start()
        gc(i).wait_recv()
        gtwo[i] = gpart[i] + gcore[i]
        gxc(i).start()
        keep[s, at] = part[s, core_of, half_of, at].astype(F32) + crecv[s, half_of, at].astype(F32)

    def give_back(i):
        s, at, _ = piece(i)
        rx(i).wait_recv()
        total = (keep[s, at] + xrecv[s, at].astype(F32)).astype(BF)
        if i == 0:
            ret[me] = total
        else:
            rsend[s, at] = total
            if i == 1:
                back(0, 1).start()
            else:
                back(i - 1, 0).start()
                back(i - 1, 1).start()
        gxc(i).wait_recv()
        summed = gtwo[i] + gx[i]
        if i == 0:
            gret[me] = summed
        else:
            gsend[i] = summed
            if i == 1:
                back_g(0, 1).start()
            else:
                back_g(i - 1, 0).start()
                back_g(i - 1, 1).start()

    for load in loads[0:2]:
        load.wait()
    tiles[z] = jnp.concatenate(
        [
            rtv[...].astype(F32),
            rwv[...].astype(BF).astype(F32),
            jnp.zeros((8 - 2 * top, tok_rows), F32),
        ],
        axis=0,
    )
    for load in loads[2:4]:
        load.wait()
    pl.semaphore_wait(
        barrier, 3 + jnp.where(z > 0, 1, 0) + jnp.where(z < planes - 1, 1, 0)
    )

    for up, there in ((True, z < planes - 1), (False, z > 0)):

        @pl.when(there)
        def _():
            zt_own(up).start()
            z_own(up, 0).start()
            z_own(up, 1).start()

    read_tile(0)
    other = cperm[0, cap:both_rows, :]
    for p in range(2):
        ysend[0, p] = dot_f32(other, xg[p, :, columns(tp)], ((1,), (0,))).astype(BF)
        yf(0, p, tp).start()
        ysend[planes, p] = dot_f32(other, xg[p, :, columns(tp_x)], ((1,), (0,))).astype(BF)
        yf(0, p, tp_x).start()
    own = cperm[0, 0:cap, :]
    for b in range(4):
        for p in range(2):
            abuf[z, b, p, rows(y)] = dot_f32(
                own, xg[p, :, b * quarter : (b + 1) * quarter], ((1,), (0,))
            ).astype(BF)
    for load in loads[4:9]:
        load.wait()
    compute(0)

    def tile_in(i):
        landed("ZT", source[i], tiles.at[source[i]])

        @pl.when(inner)
        def _():
            zt_relay(i).start()

    tile_in(1)
    pl.when(inner)(functools.partial(tile_in, 2))
    read_tile(1)
    ohid_ref[...] = dot_f32(xg[1], sdv[...], ((1,), (0,))).astype(BF)
    rows_each = feat // n
    for j in range(n):
        ssend[j % 2, j // 2] = dot_f32(
            xg[1, :, j * rows_each : (j + 1) * rows_each], shv[...], ((0,), (0,))
        ).astype(BF)

    take(1, 0)
    take(2, 0, inner)
    spread(1, 0)
    core_sum(0)
    pair(0).start()
    take(1, 1)
    take(2, 1, inner)
    spread(1, 1)
    pair(1).start()
    landed("Y0", 0, abuf.at[z, 0:2, :, rows(1 - y)])
    for p in range(2):
        to_core(0, p, tp).start()
        to_core(0, p, tp_x).start()
    pl.when(inner)(functools.partial(tile_in, 3))
    crossed(1)
    ready(0)
    compute(1)
    pl.when(outer)(functools.partial(tile_in, 2))
    take(2, 0, outer)
    read_tile(2)
    take(3, 0, inner)
    spread(2, 0)
    pair(2).start()
    joined(1, 0)
    core_sum(1)
    take(2, 1, outer)
    take(3, 1, inner)
    spread(2, 1)
    pair(3).start()
    joined(1, 1)
    crossed(2)

    ready(1)
    compute(2)
    give_back(0)
    pl.when(outer)(functools.partial(tile_in, 3))
    take(3, 0, outer)
    read_tile(3)
    spread(3, 0)
    core_sum(2)
    joined(2, 0)
    take(3, 1, outer)
    spread(3, 1)
    joined(2, 1)
    give_back(1)
    crossed(3)
    ready(2)
    compute(3)

    names = lax.broadcasted_iota(jnp.int32, (128, tok_rows), 0)
    named_t = jnp.zeros((128, tok_rows), F32)
    for k in range(top):
        named_t = named_t + jnp.where(rtv[k : k + 1, :] == names, 1.0, 0.0)
    rank_t = dot_f32(named_t.astype(BF), before, ((1,), (0,)))
    for e in range(n):
        perm[e] = jnp.where(slot == rank_t[e : e + 1, :], named_t[e : e + 1, :], 0.0).astype(BF)

    give_back(2)
    core_sum(3)
    landed("PAIR", 0, spair)
    for q in range(planes):
        ssum[q] = (ssend[y, q].astype(F32) + spair[q].astype(F32)).astype(BF)
    srecv[z] = ssum[z]
    for d in range(1, planes):
        share(d).start()
    joined(3, 0)
    joined(3, 1)
    ready(3)
    compute(4)
    give_back(3)
    core_sum(4)

    d_all = dgu[...].reshape(n * cap, 2 * units)
    h_all = hw[...].reshape(n * cap, units)
    for b in range(4):
        at = slice(b * quarter, (b + 1) * quarter)
        grad = dot_f32(abuf[:, b, 0].reshape(n * cap, quarter), d_all, ((0,), (0,))).astype(BF)
        gradv[0, at, :] = grad[:, 0:units]
        gradv[1, at, :] = grad[:, units : 2 * units]
        wdv[:, at] = dot_f32(
            h_all, abuf[:, b, 1].reshape(n * cap, quarter), ((0,), (0,))
        ).astype(BF)

    stores = [
        pltpu.make_async_copy(gradv.at[0], og_ref, store_sem.at[0]),
        pltpu.make_async_copy(gradv.at[1], ou_ref, store_sem.at[1]),
        pltpu.make_async_copy(wdv, od_ref, store_sem.at[2]),
    ]
    for store in stores:
        store.start()

    give_back(4)

    landed("SHARE", 0, srecv.at[0 : planes - 1])
    sums = srecv[0].astype(F32)
    for j in range(1, planes):
        sums = sums + srecv[j].astype(F32)
    osh_ref[...] = sums

    landed("RG", 0, gret.at[0 : n - 1])
    pieces = []
    for e in range(n):
        full = gret[e]
        row = jnp.where(at_zero, full[:, 0:cap], full[:, cap:both_rows]).astype(BF)
        pieces.append(dot_f32(row, perm[e], ((1,), (0,)))[0:1, :])
    pieces.append(jnp.zeros((128 - n, tok_rows), F32))
    values = jnp.concatenate(pieces, axis=0)
    for k in range(top):
        hit = rtv[k : k + 1, :] == names
        ow_ref[k : k + 1, :] = jnp.sum(jnp.where(hit, values, 0.0), axis=0, keepdims=True)

    landed("RE", 0, ret.at[0 : n - 1])
    otok_ref[...] = dot_f32(
        perm[...].reshape(n * cap, tok_rows), ret[...].reshape(n * cap, quarter), ((0,), (0,))
    ).astype(BF)

    for store in stores:
        store.wait()

    @pl.when(inner)
    def _():
        left(S_ZO, zbuf.at[0:2])
        left(S_TO, tiles.at[0:2])
        left(S_ZR, zbuf.at[0 : planes - 1])
        left(S_TR, tiles.at[0 : planes - 1])

    @pl.when(outer)
    def _():
        left(S_ZO, zbuf.at[0:1])
        left(S_TO, tiles.at[0:1])

    left(S_Y, ysend)
    left(S_YW, wysend)
    left(S_FX, zbuf.at[0 : planes - 1])
    left(S_C0, abuf.at[0, 0:2, :, 0:cap])
    left(S_C, abuf.at[0 : planes - 1, 0:2])
    left(S_RC, crecv)
    left(S_RX, xsend)
    left(S_GC, gpart)
    left(S_GX, gtwo)
    left(S_RE, ret.at[0 : n - 1])
    left(S_RG, gret.at[0 : n - 1])
    left(S_SHARE, srecv.at[0 : planes - 1])
    left(S_PAIR, spair)


def pass_on(*refs):
    count = (len(refs) - 2) // 3
    ins, outs, held = refs[:count], refs[count : 2 * count], refs[2 * count : 3 * count]
    in_sem, out_sem = refs[-2:]
    loads = [pltpu.make_async_copy(ins[i], held[i], in_sem.at[i]) for i in range(count)]
    stores = [pltpu.make_async_copy(held[i], outs[i], out_sem.at[i]) for i in range(count)]
    for load in loads:
        load.start()
    for load, store in zip(loads, stores):
        load.wait()
        store.start()
    for store in stores:
        store.wait()


def hand_over(arrays):
    count = len(arrays)
    hbm = pl.BlockSpec(memory_space=pl.ANY)
    return pl.pallas_call(
        pass_on,
        out_shape=tuple(jax.ShapeDtypeStruct(a.shape, a.dtype) for a in arrays),
        in_specs=[hbm] * count,
        out_specs=tuple([hbm] * count),
        scratch_shapes=[pltpu.VMEM(a.shape, a.dtype) for a in arrays]
        + [pltpu.SemaphoreType.DMA((count,))] * 2,
    )(*arrays)


def fused_shards(
    tokens,
    cotangent,
    route_weights,
    routes,
    gate_proj,
    up_proj,
    down_proj,
    shared_down,
    shared_hidden,
):
    n = lax.axis_size("ep")
    tok_rows, feat = tokens.shape
    top = routes.shape[1]
    units = gate_proj.shape[2]
    hid = shared_hidden.shape[1]
    cap = 2 * tok_rows * top // n
    quarter = feat // 4
    planes = n // 2
    out_shape = (
        jax.ShapeDtypeStruct((tok_rows, quarter), BF),
        jax.ShapeDtypeStruct((top, tok_rows), F32),
        jax.ShapeDtypeStruct((feat, units), BF),
        jax.ShapeDtypeStruct((feat, units), BF),
        jax.ShapeDtypeStruct((units, feat), BF),
        jax.ShapeDtypeStruct((tok_rows, hid), BF),
        jax.ShapeDtypeStruct((feat // n, hid), F32),
    )
    vmem = pl.BlockSpec(memory_space=pltpu.VMEM)
    hbm = pl.BlockSpec(memory_space=pl.ANY)
    per_piece = pltpu.VMEM((planes + 1, 8, 128), F32)
    outs = pl.pallas_call(
        functools.partial(kernel, n, cap),
        out_shape=out_shape,
        in_specs=[hbm] * 9,
        out_specs=(vmem, vmem, hbm, hbm, hbm, vmem, vmem),
        scratch_shapes=[
            pltpu.VMEM((2, tok_rows, feat), BF),
            pltpu.VMEM((top, tok_rows), F32),
            pltpu.VMEM((top, tok_rows), jnp.int32),
            pltpu.VMEM((tok_rows, hid), BF),
            pltpu.VMEM((planes, 2, tok_rows, quarter), BF),
            pltpu.VMEM((planes, 8, tok_rows), F32),
            pltpu.VMEM((planes, 2 * cap, tok_rows), BF),
            pltpu.VMEM((n, cap, tok_rows), BF),
            pltpu.VMEM((planes + 1, 2, cap, quarter), BF),
            pltpu.VMEM((planes, 8, 2 * cap), F32),
            pltpu.VMEM((n, 8, 2 * cap), F32),
            pltpu.VMEM((planes, 4, 2, 2 * cap, quarter), BF),
            pltpu.VMEM((feat, 2 * units), BF),
            pltpu.VMEM((units, feat), BF),
            pltpu.VMEM((feat, hid), BF),
            pltpu.VMEM((2, feat, units), BF),
            pltpu.VMEM((planes, 2 * cap, units), BF),
            pltpu.VMEM((planes, 2 * cap, 2 * units), BF),
            pltpu.VMEM((planes, 2, 2, 2 * cap, quarter), BF),
            pltpu.VMEM((planes, 2, 2 * cap, quarter), BF),
            pltpu.VMEM((planes, 2 * cap, quarter), F32),
            pltpu.VMEM((planes, 2 * cap, quarter), BF),
            pltpu.VMEM((planes, 2 * cap, quarter), BF),
            pltpu.VMEM((planes, 2 * cap, quarter), BF),
            pltpu.VMEM((n, cap, quarter), BF),
            per_piece,
            per_piece,
            per_piece,
            per_piece,
            per_piece,
            pltpu.VMEM((n, 8, 128), F32),
            pltpu.VMEM((2, planes, feat // n, hid), BF),
            pltpu.VMEM((planes, feat // n, hid), BF),
            pltpu.VMEM((planes, feat // n, hid), BF),
            pltpu.VMEM((planes, feat // n, hid), BF),
            pltpu.SemaphoreType.DMA((SENDS,)),
            pltpu.SemaphoreType.DMA((ARRIVALS,)),
            pltpu.SemaphoreType.DMA((9,)),
            pltpu.SemaphoreType.DMA((3,)),
        ],
        compiler_params=pltpu.CompilerParams(
            collective_id=0, has_side_effects=True, vmem_limit_bytes=60 * 1024 * 1024
        ),
    )(
        tokens,
        cotangent,
        route_weights.T,
        routes.T,
        gate_proj[0],
        up_proj[0],
        down_proj[0],
        shared_down,
        shared_hidden,
    )
    outs = hand_over(outs)
    return outs[0], outs[1].T, outs[2][None], outs[3][None], outs[4][None], outs[5], outs[6]


def shards(*args):
    tokens, routes, gate_proj = args[0], args[3], args[4]
    n = lax.axis_size("ep")
    tok_rows, feat = tokens.shape
    top = routes.shape[1]
    fits = (
        gate_proj.shape[0] == 1
        and lax.axis_size("tp") == 4
        and n == 8
        and tok_rows == 128
        and 4 * tok_rows * top == n * tok_rows
        and 2 * top <= 8
        and feat % 512 == 0
        and feat // n % 128 == 0
    )
    if fits:
        return fused_shards(*args)
    return plain_shards(*args)


def plain_shards(
    tokens,
    cotangent,
    route_weights,
    routes,
    gate_proj,
    up_proj,
    down_proj,
    shared_down,
    shared_hidden,
):
    tok_rows, feat_width = tokens.shape
    top_count = routes.shape[1]
    exp_local = gate_proj.shape[0]
    ep_size = lax.axis_size("ep")
    tp_size = lax.axis_size("tp")
    exp_total = exp_local * ep_size
    capacity = 2 * tok_rows * top_count // exp_total
    quarter = feat_width // tp_size
    filled = exp_total * capacity
    flat_routes = routes.reshape(-1)
    one_hot = (flat_routes[:, None] == jnp.arange(exp_total, dtype=jnp.int32)[None, :]).astype(
        jnp.int32
    )
    rank_in = jnp.sum((jnp.cumsum(one_hot, axis=0) - one_hot) * one_hot, axis=1)
    slot_ids = flat_routes * capacity + rank_in
    route_owner = jnp.arange(flat_routes.shape[0], dtype=jnp.int32) // top_count
    owner_ids = jnp.full((filled,), tok_rows, jnp.int32).at[slot_ids].set(route_owner)
    sent_weights = (
        jnp.zeros((filled,), jnp.bfloat16)
        .at[slot_ids]
        .set(route_weights.reshape(-1).astype(jnp.bfloat16))
    )
    first_col = lax.axis_index("tp") * quarter
    own_rows = lax.dynamic_slice_in_dim(tokens, first_col, quarter, 1)
    own_grads = lax.dynamic_slice_in_dim(cotangent, first_col, quarter, 1)
    sent_rows = jnp.take(own_rows, owner_ids, axis=0, mode="fill", fill_value=0)
    sent_grads = jnp.take(own_grads, owner_ids, axis=0, mode="fill", fill_value=0)
    got_rows, got_grads, got_weights = (
        lax.all_to_all(sent_rows, "ep", split_axis=0, concat_axis=0, tiled=True),
        lax.all_to_all(sent_grads, "ep", split_axis=0, concat_axis=0, tiled=True),
        lax.all_to_all(sent_weights, "ep", split_axis=0, concat_axis=0, tiled=True),
    )
    got_rows, got_grads = (
        lax.all_gather(got_rows, "tp", axis=1, tiled=True),
        lax.all_gather(got_grads, "tp", axis=1, tiled=True),
    )
    slot_rows = got_rows.reshape(ep_size, exp_local, capacity, feat_width)
    slot_grads = got_grads.reshape(ep_size, exp_local, capacity, feat_width)
    weight_col = got_weights.reshape(ep_size, exp_local, capacity, 1).astype(jnp.float32)
    gate = jnp.einsum("secd,edf->secf", slot_rows, gate_proj, preferred_element_type=jnp.float32)
    upper = jnp.einsum("secd,edf->secf", slot_rows, up_proj, preferred_element_type=jnp.float32)
    active = jax.nn.silu(gate)
    hidden = (active * upper).astype(jnp.bfloat16)
    backed = jnp.einsum("secd,efd->secf", slot_grads, down_proj, preferred_element_type=jnp.float32)
    gate_share = jnp.sum(hidden.astype(jnp.float32) * backed, axis=3)
    d_hidden = weight_col * backed
    sigma = jax.nn.sigmoid(gate)
    d_gate = (d_hidden * upper * sigma * (1.0 + gate * (1.0 - sigma))).astype(jnp.bfloat16)
    d_up = (d_hidden * active).astype(jnp.bfloat16)
    scaled = (weight_col * slot_grads).astype(jnp.bfloat16)
    down_proj_grad = jnp.einsum(
        "secf,secd->efd", hidden, scaled, preferred_element_type=jnp.float32
    ).astype(jnp.bfloat16)
    gate_proj_grad = jnp.einsum(
        "secd,secf->edf", slot_rows, d_gate, preferred_element_type=jnp.float32
    ).astype(jnp.bfloat16)
    up_proj_grad = jnp.einsum(
        "secd,secf->edf", slot_rows, d_up, preferred_element_type=jnp.float32
    ).astype(jnp.bfloat16)
    partial_value = jnp.einsum(
        "secf,edf->secd", d_gate, gate_proj, preferred_element_type=jnp.float32
    )
    partial_value = partial_value + jnp.einsum(
        "secf,edf->secd", d_up, up_proj, preferred_element_type=jnp.float32
    )
    gate_whole = lax.psum(gate_share, "tp")
    input_cols = lax.psum_scatter(
        partial_value.astype(jnp.bfloat16), "tp", scatter_dimension=3, tiled=True
    )
    back_cols, back_gate = (
        lax.all_to_all(
            input_cols.reshape(filled, quarter), "ep", split_axis=0, concat_axis=0, tiled=True
        ),
        lax.all_to_all(
            gate_whole.astype(jnp.bfloat16).reshape(filled),
            "ep",
            split_axis=0,
            concat_axis=0,
            tiled=True,
        ),
    )
    picked = back_cols[slot_ids].reshape(tok_rows, top_count, quarter)
    tokens_grad = jnp.sum(picked.astype(jnp.float32), axis=1).astype(jnp.bfloat16)
    weights_grad = back_gate[slot_ids].astype(jnp.float32).reshape(tok_rows, top_count)
    hidden_grad = jnp.dot(cotangent, shared_down, preferred_element_type=jnp.float32).astype(
        jnp.bfloat16
    )
    shared_grad = lax.psum_scatter(
        jnp.einsum("td,th->dh", cotangent, shared_hidden, preferred_element_type=jnp.float32),
        "ep",
        scatter_dimension=0,
        tiled=True,
    )
    return (
        tokens_grad,
        weights_grad,
        gate_proj_grad,
        up_proj_grad,
        down_proj_grad,
        hidden_grad,
        shared_grad,
    )


def solution(mesh):
    in_specs = (
        P("ep", None),
        P("ep", None),
        P("ep", None),
        P("ep", None),
        P("ep", None, "tp"),
        P("ep", None, "tp"),
        P("ep", "tp", None),
        P(None, "tp"),
        P("ep", "tp"),
    )
    out_specs = (
        P("ep", "tp"),
        P("ep", None),
        P("ep", None, "tp"),
        P("ep", None, "tp"),
        P("ep", "tp", None),
        P("ep", "tp"),
        P("ep", "tp"),
    )
    return jax.shard_map(shards, mesh=mesh, in_specs=in_specs, out_specs=out_specs, check_vma=False)
```

```python
import functools

import jax
import jax.numpy as jnp
from jax import lax
from jax.experimental import pallas as pl
from jax.experimental.pallas import tpu as pltpu
from jax.sharding import PartitionSpec as P

MESH = pl.DeviceIdType.MESH
BF = jnp.bfloat16
F32 = jnp.float32
S_ZO, S_ZR, S_TO, S_TR, S_Y, S_YW, S_FX, S_C0, S_C = range(9)
S_RC, S_RX, S_GC, S_GX, S_RE, S_RG, S_SHARE, S_PAIR, SENDS = range(9, 18)
COUNTS = {
    "ZF": 16,
    "ZT": 4,
    "Y0": 1,
    "YF": 12,
    "YW": 4,
    "FX": 12,
    "CORE": 4,
    "RC": 5,
    "RX": 6,
    "GC": 5,
    "GX": 5,
    "RE": 1,
    "RG": 1,
    "SHARE": 1,
    "PAIR": 1,
}
FIRST = {kind: sum(list(COUNTS.values())[:i]) for i, kind in enumerate(COUNTS)}
ARRIVALS = sum(COUNTS.values())


def dot_f32(a, b, dims):
    return lax.dot_general(a, b, (dims, ((), ())), preferred_element_type=F32)


def kernel(
    n,
    cap,
    tok_ref,
    cot_ref,
    rw_ref,
    rt_ref,
    wg_ref,
    wu_ref,
    wd_ref,
    sd_ref,
    sh_ref,
    otok_ref,
    ow_ref,
    og_ref,
    ou_ref,
    od_ref,
    ohid_ref,
    osh_ref,
    xg,
    rwv,
    rtv,
    shv,
    zbuf,
    tiles,
    cperm,
    perm,
    ysend,
    wysend,
    wrecv,
    abuf,
    wgu,
    wdv,
    sdv,
    hw,
    dgu,
    part,
    crecv,
    keep,
    xsend,
    xrecv,
    rsend,
    ret,
    gpart,
    gcore,
    gtwo,
    gx,
    gsend,
    gret,
    ssend,
    spair,
    ssum,
    srecv,
    send_sem,
    recv_sem,
    load_sem,
):
    me = lax.axis_index("ep")
    tp = lax.axis_index("tp")
    tok_rows, feat = tok_ref.shape
    top = rt_ref.shape[0]
    quarter = feat // 4
    units = wg_ref.shape[1]
    planes = n // 2
    both_rows = 2 * cap
    y = lax.rem(me, 2)
    z = me // 2
    core_of = lax.rem(tp, 2)
    half_of = tp // 2
    tp_c = half_of * 2 + (1 - core_of)
    tp_x = (1 - half_of) * 2 + core_of
    tp_xc = (1 - half_of) * 2 + (1 - core_of)
    me_y = jnp.bitwise_xor(me, 1)
    inner = (z > 0) & (z < planes - 1)
    outer = (z == 0) | (z == planes - 1)
    low_inner = z == 1
    high_inner = z == planes - 2
    first = jnp.where(z == 0, 1, z - 1)
    second = jnp.where(z == 0, 2, jnp.where(low_inner, z + 1, 0))
    source = [z, first, second, jnp.where(z == planes - 1, 1, planes - 1)]
    pieces_of = range(4)
    part_cols = quarter // 2

    def copy(out, kind, at, src_ref, dst_ref, ep_to, tp_to):
        return pltpu.make_async_remote_copy(
            src_ref=src_ref,
            dst_ref=dst_ref,
            send_sem=send_sem.at[out],
            recv_sem=recv_sem.at[FIRST[kind] + at],
            device_id=(ep_to, tp_to),
            device_id_type=MESH,
        )

    def landed(kind, at, whole_ref):
        copy(0, kind, at, whole_ref, whole_ref, me_y, tp).wait_recv()

    def left(out, whole_ref):
        copy(out, "ZT", 0, whole_ref, whole_ref, me_y, tp).wait_send()

    def rows(block_y):
        return pl.ds(pl.multiple_of(block_y * cap, cap), cap)

    def split(c):
        return c // 2, pl.ds((c % 2) * part_cols, part_cols)

    def columns(block):
        return pl.ds(pl.multiple_of(block * quarter, quarter), quarter)

    barrier = pltpu.get_barrier_semaphore()
    for to in ((me_y, tp), (me, tp_c), (me, tp_x)):
        pl.semaphore_signal(barrier, inc=1, device_id=to, device_id_type=MESH)

    @pl.when(z > 0)
    def _():
        pl.semaphore_signal(barrier, inc=1, device_id=(me - 2, tp), device_id_type=MESH)

    @pl.when(z < planes - 1)
    def _():
        pl.semaphore_signal(barrier, inc=1, device_id=(me + 2, tp), device_id_type=MESH)

    loads = [
        pltpu.make_async_copy(src, dst, load_sem.at[i])
        for i, (src, dst) in enumerate(
            (
                (rt_ref, rtv),
                (rw_ref, rwv),
                (tok_ref, xg.at[0]),
                (cot_ref, xg.at[1]),
                (wg_ref, wgu.at[:, pl.ds(0, units)]),
                (wu_ref, wgu.at[:, pl.ds(units, units)]),
                (wd_ref, wdv),
                (sd_ref, sdv),
                (sh_ref, shv),
            )
        )
    ]
    for load in loads:
        load.start()

    before = jnp.where(
        lax.broadcasted_iota(jnp.int32, (tok_rows, tok_rows), 0)
        < lax.broadcasted_iota(jnp.int32, (tok_rows, tok_rows), 1),
        1.0,
        0.0,
    ).astype(BF)
    slot = lax.broadcasted_iota(jnp.int32, (cap, tok_rows), 0).astype(F32)
    two = jnp.where(
        lax.broadcasted_iota(jnp.int32, (8, tok_rows), 0) == 0,
        me.astype(F32),
        me_y.astype(F32),
    )
    at_zero = y == 0

    def place(values):
        low = jnp.where(at_zero, values, 0.0)
        return jnp.concatenate([low, values - low], axis=1)

    def read_tile(i):
        s = source[i]
        named = jnp.zeros((8, tok_rows), F32)
        weight = jnp.zeros((8, tok_rows), F32)
        for k in range(top):
            hit = tiles[s, k : k + 1, :] == two
            named = named + jnp.where(hit, 1.0, 0.0)
            weight = weight + jnp.where(hit, tiles[s, top + k : top + k + 1, :], 0.0)
        rank = dot_f32(named.astype(BF), before, ((1,), (0,)))
        picks = jnp.concatenate(
            [
                jnp.where(slot == rank[j : j + 1, :], named[j : j + 1, :], 0.0).astype(BF)
                for j in range(2)
            ],
            axis=0,
        )
        cperm[i] = picks
        slotted = dot_f32(weight.astype(BF), picks, ((1,), (1,)))
        wrecv[2 * s + y] = jnp.broadcast_to(place(slotted[0:1, 0:cap]), (8, both_rows))
        wysend[i] = jnp.broadcast_to(place(slotted[1:2, cap:both_rows]), (8, both_rows))
        copy(S_YW, "YW", i, wysend.at[i], wrecv.at[2 * s + y], me_y, tp).start()

    def yw_in(i):
        at = 2 * source[i] + (1 - y)
        return copy(S_YW, "YW", i, wrecv.at[at], wrecv.at[at], me_y, tp)

    def yf(i, c):
        p, at = split(c)
        dst = abuf.at[source[i], tp, p, rows(y), at]
        return copy(S_Y, "YF", 4 * (i - 1) + c, ysend.at[i, p, :, at], dst, me_y, tp)

    def y_own(c, block):
        p, at = split(c)
        src = ysend.at[planes if block is tp_x else 0, p, :, at]
        return copy(S_Y, "Y0", 0, src, abuf.at[z, block, p, rows(y), at], me_y, tp)


    def z_own(up, c):
        to = me + 2 if up else me - 2
        p, at = split(c)
        first = pl.multiple_of(tp * quarter + (c % 2) * part_cols, part_cols)
        src = xg.at[p, :, pl.ds(first, part_cols)]
        return copy(S_ZO, "ZF", 4 * z + c, src, zbuf.at[z, p, :, at], to, tp)

    def zt_own(up):
        to = me + 2 if up else me - 2
        return copy(S_TO, "ZT", z, tiles.at[z], tiles.at[z], to, tp)

    def z_relay(i, c):
        s = source[i]
        to = jnp.where(s < z, me + 2, me - 2)
        p, at = split(c)
        block = zbuf.at[s, p, :, at]
        return copy(S_ZR, "ZF", 4 * s + c, block, block, to, tp)

    def zt_relay(i):
        s = source[i]
        to = jnp.where(s < z, me + 2, me - 2)
        return copy(S_TR, "ZT", s, tiles.at[s], tiles.at[s], to, tp)

    def fx(i, j, c):
        block_y = y if j == 0 else 1 - y
        p, at = split(c)
        block = abuf.at[source[i], tp, p, rows(block_y), at]
        return copy(S_FX, "FX", 4 * (i - 1) + c, block, block, me, tp_x)

    def own_to_core(p, block):
        at = abuf.at[z, block, p, rows(1 - y)]
        return copy(S_C0, "CORE", 0, at, at, me, tp_c)

    def to_core(i, c, block):
        p, at = split(c)
        part_of = abuf.at[source[i], block, p, :, at]
        return copy(S_C, "CORE", i, part_of, part_of, me, tp_c)

    rows_each = feat // n

    def pair(q):
        at = pl.ds((q % 2) * (rows_each // 2), rows_each // 2)
        src = ssend.at[1 - y, q // 2, at]
        return copy(S_PAIR, "PAIR", 0, src, spair.at[q // 2, at], me_y, tp)

    def share(d):
        to = jnp.bitwise_xor(z, d)
        return copy(S_SHARE, "SHARE", 0, ssum.at[to], srecv.at[z], 2 * to + y, tp)

    def piece(i):
        if i == 0:
            return z, rows(y), cap
        if i == 1:
            return z, rows(1 - y), cap
        return source[i - 1], pl.ds(0, both_rows), both_rows

    def rc(i):
        s, at, _ = piece(i)
        return copy(S_RC, "RC", i, part.at[s, 1 - core_of, :, at], crecv.at[s, :, at], me, tp_c)

    def rx(i, j=None):
        s, at, _ = piece(i)
        if j is not None:
            at = rows(y if j == 0 else 1 - y)
        return copy(S_RX, "RX", i + (j or 0), xsend.at[s, at], xrecv.at[s, at], me, tp_x)

    def gc(i):
        return copy(S_GC, "GC", i, gpart.at[i, 0:1], gcore.at[i, 0:1], me, tp_c)

    def gxc(i):
        return copy(S_GX, "GX", i, gtwo.at[i, 0:1], gx.at[i, 0:1], me, tp_x)

    def back(i, j):
        s = source[i]
        block_y = y if j == 0 else 1 - y
        return copy(
            S_RE, "RE", 0, rsend.at[s, rows(block_y)], ret.at[me], 2 * s + block_y, tp
        )

    def back_g(i, j):
        to = 2 * source[i] + (y if j == 0 else 1 - y)
        return copy(S_RG, "RG", 0, gsend.at[i + 1, 0:1], gret.at[me, 0:1], to, tp)

    def take(i, c, gate=None):
        def run():
            p, at = split(c)
            landed("ZF", 4 * source[i] + c, zbuf.at[source[i], p, :, at])

            @pl.when(low_inner if i == 1 else inner)
            def _():
                z_relay(i, c).start()

        if gate is None:
            run()
        else:
            pl.when(gate)(run)

    def spread(i, c):
        p, at = split(c)
        moved = dot_f32(cperm[i], zbuf[source[i], p, :, at], ((1,), (0,))).astype(BF)
        abuf[source[i], tp, p, rows(y), at] = moved[0:cap]
        ysend[i, p, :, at] = moved[cap:both_rows]
        yf(i, c).start()
        fx(i, 0, c).start()

    def crossed(i, c):
        p, at = split(c)
        landed("YF", 4 * (i - 1) + c, abuf.at[source[i], tp, p, rows(1 - y), at])
        fx(i, 1, c).start()
        to_core(i, c, tp).start()

    def ready(i):
        yw_in(i).wait_recv()
        if i == 0:
            landed("CORE", 0, abuf.at[z, 0:2, :, rows(1 - y)])
        else:
            landed("CORE", i, abuf.at[source[i], 0:2])

    def joined(i, c):
        p, at = split(c)
        landed("FX", 4 * (i - 1) + c, abuf.at[source[i], tp_x, p, :, at])
        to_core(i, c, tp_x).start()

    def compute(i):
        s, at, m = piece(i)
        both = jnp.zeros((m, 2 * units), F32)
        backed = jnp.zeros((m, units), F32)
        for b in range(4):
            cols = slice(b * quarter, (b + 1) * quarter)
            both = both + dot_f32(abuf[s, b, 0, at], wgu[cols, :], ((1,), (0,)))
            backed = backed + dot_f32(abuf[s, b, 1, at], wdv[:, cols], ((1,), (1,)))
        gate = both[:, 0:units]
        upper = both[:, units : 2 * units]
        sigma = jax.nn.sigmoid(gate)
        active = gate * sigma
        hidden = (active * upper).astype(BF).astype(F32)
        if i == 0:
            wrow, first = wrecv[me, 0:1, :], y * cap
        elif i == 1:
            wrow, first = wrecv[me_y, 0:1, :], (1 - y) * cap
        else:
            wrow, first = wrecv[2 * s, 0:1, :] + wrecv[2 * s + 1, 0:1, :], 0
        eye = (
            lax.broadcasted_iota(jnp.int32, (m, both_rows), 0) + first
            == lax.broadcasted_iota(jnp.int32, (m, both_rows), 1)
        )
        wcol = jnp.sum(jnp.where(eye, wrow, 0.0), axis=1, keepdims=True)
        d_hidden = wcol * backed
        hw[s, at] = (wcol * hidden).astype(BF)
        d_both = jnp.concatenate(
            [
                (d_hidden * upper * sigma * (1.0 + gate * (1.0 - sigma))).astype(BF),
                (d_hidden * active).astype(BF),
            ],
            axis=1,
        )
        dgu[s, at] = d_both
        for b in range(4):
            cols = slice(b * quarter, (b + 1) * quarter)
            part[s, b % 2, b // 2, at] = dot_f32(d_both, wgu[cols, :], ((1,), (1,))).astype(BF)
        rc(i).start()
        sums = lax.dot_general(
            jnp.ones((8, units), F32),
            hidden * backed,
            (((1,), (1,)), ((), ())),
            precision=lax.Precision.HIGHEST,
            preferred_element_type=F32,
        )
        if i == 0:
            sums = place(sums)
        elif i == 1:
            low = jnp.where(at_zero, 0.0, sums)
            sums = jnp.concatenate([low, sums - low], axis=1)
        gpart[i] = sums
        gc(i).start()

    def core_sum(i):
        s, whole, _ = piece(i)
        rc(i).wait_recv()
        for j in (0, 1) if i == planes else (None,):
            at = whole if j is None else rows(y if j == 0 else 1 - y)
            xsend[s, at] = (
                part[s, core_of, 1 - half_of, at].astype(F32)
                + crecv[s, 1 - half_of, at].astype(F32)
            ).astype(BF)
            rx(i, j).start()
        gc(i).wait_recv()
        gtwo[i, 0:1] = gpart[i, 0:1] + gcore[i, 0:1]
        gxc(i).start()
        keep[s, whole] = part[s, core_of, half_of, whole].astype(F32) + crecv[
            s, half_of, whole
        ].astype(F32)

    def give_back(i):
        s, whole, _ = piece(i)
        if i == planes:
            for j in range(2):
                at = rows(y if j == 0 else 1 - y)
                rx(i, j).wait_recv()
                rsend[s, at] = (keep[s, at] + xrecv[s, at].astype(F32)).astype(BF)
                back(i - 1, j).start()
        else:
            rx(i).wait_recv()
            total = (keep[s, whole] + xrecv[s, whole].astype(F32)).astype(BF)
            if i == 0:
                ret[me] = total
            else:
                rsend[s, whole] = total
                for j in (1,) if i == 1 else (0, 1):
                    back(max(i - 1, 0), j).start()
        gxc(i).wait_recv()
        summed = gtwo[i, 0:1] + gx[i, 0:1]
        if i == 0:
            gret[me, 0:1] = summed
        else:
            gsend[i, 0:1] = summed
            for j in (1,) if i == 1 else (0, 1):
                back_g(i - 1, j).start()

    for load in loads[0:2]:
        load.wait()
    tiles[z] = jnp.concatenate(
        [
            rtv[...].astype(F32),
            rwv[...].astype(BF).astype(F32),
            jnp.zeros((8 - 2 * top, tok_rows), F32),
        ],
        axis=0,
    )
    for load in loads[2:4]:
        load.wait()
    pl.semaphore_wait(
        barrier, 3 + jnp.where(z > 0, 1, 0) + jnp.where(z < planes - 1, 1, 0)
    )

    for up, there in ((True, z < planes - 1), (False, z > 0)):

        @pl.when(there)
        def _():
            zt_own(up).start()
            for c in pieces_of:
                z_own(up, c).start()

    read_tile(0)
    loads[8].wait()
    for j in range(n):
        ssend[j % 2, j // 2] = dot_f32(
            xg[1, :, j * rows_each : (j + 1) * rows_each], shv[...], ((0,), (0,))
        ).astype(BF)
    for q in range(planes):
        pair(q).start()
    other = cperm[0, cap:both_rows, :]
    for p in range(2):
        ysend[0, p] = dot_f32(other, xg[p, :, columns(tp)], ((1,), (0,))).astype(BF)
        ysend[planes, p] = dot_f32(other, xg[p, :, columns(tp_x)], ((1,), (0,))).astype(BF)
    own = cperm[0, 0:cap, :]
    for b in range(4):
        for p in range(2):
            abuf[z, b, p, rows(y)] = dot_f32(
                own, xg[p, :, b * quarter : (b + 1) * quarter], ((1,), (0,))
            ).astype(BF)
    for load in loads[4:8]:
        load.wait()
    compute(0)

    def tile_in(i):
        landed("ZT", source[i], tiles.at[source[i]])

        @pl.when(inner)
        def _():
            zt_relay(i).start()

    late_second = jnp.logical_not(low_inner)
    late_third = jnp.logical_not(high_inner)
    tile_in(1)
    pl.when(low_inner)(functools.partial(tile_in, 2))
    pl.when(high_inner)(functools.partial(tile_in, 3))
    read_tile(1)
    ohid_ref[...] = dot_f32(xg[1], sdv[...], ((1,), (0,))).astype(BF)
    core_sum(0)
    for c in pieces_of:
        take(1, c)
        take(2, c, low_inner)
        take(3, c, high_inner)
        spread(1, c)
    for q in range(planes, 2 * planes):
        pair(q).start()
    pl.when(late_second)(functools.partial(tile_in, 2))
    crossed(1, 0)
    read_tile(2)
    for c in pieces_of:
        take(2, c, late_second)
        spread(2, c)
        if c < 3:
            crossed(1, c + 1)

    @pl.when(high_inner)
    def _():
        for c in pieces_of:
            z_relay(1, c).start()

    pl.when(late_third)(functools.partial(tile_in, 3))
    read_tile(3)
    joined(1, 0)
    joined(1, 1)
    for c in pieces_of:
        crossed(2, c)
        take(3, c, late_third)
        spread(3, c)
        if c < 2:
            joined(1, c + 2)
    for c in pieces_of:
        y_own(c, tp).start()
        y_own(c, tp_x).start()
    ready(1)
    compute(2)
    joined(2, 0)
    joined(2, 1)
    crossed(3, 0)
    joined(2, 2)
    crossed(3, 1)
    joined(2, 3)
    crossed(3, 2)
    crossed(3, 3)
    core_sum(2)
    landed("PAIR", 0, spair)
    for q in range(planes):
        ssum[q] = (ssend[y, q].astype(F32) + spair[q].astype(F32)).astype(BF)
    srecv[z] = ssum[z]
    for d in range(1, planes):
        share(d).start()
    ready(2)
    compute(3)
    give_back(0)

    names = lax.broadcasted_iota(jnp.int32, (128, tok_rows), 0)
    named_t = jnp.zeros((128, tok_rows), F32)
    for k in range(top):
        named_t = named_t + jnp.where(rtv[k : k + 1, :] == names, 1.0, 0.0)
    rank_t = dot_f32(named_t.astype(BF), before, ((1,), (0,)))
    for e in range(n):
        perm[e] = jnp.where(slot == rank_t[e : e + 1, :], named_t[e : e + 1, :], 0.0).astype(BF)

    core_sum(3)
    for c in pieces_of:
        joined(3, c)
    ready(3)
    compute(4)
    give_back(2)
    core_sum(4)
    landed("Y0", 0, abuf.at[z, 0:2, :, rows(1 - y)])
    for p in range(2):
        own_to_core(p, tp).start()
        own_to_core(p, tp_x).start()
    give_back(3)
    ready(0)
    compute(1)
    core_sum(1)

    d_all = dgu[...].reshape(n * cap, 2 * units)
    h_all = hw[...].reshape(n * cap, units)
    for b in range(4):
        at = slice(b * quarter, (b + 1) * quarter)
        grad = dot_f32(abuf[:, b, 0].reshape(n * cap, quarter), d_all, ((0,), (0,))).astype(BF)
        og_ref[at, :] = grad[:, 0:units]
        ou_ref[at, :] = grad[:, units : 2 * units]
        od_ref[:, at] = dot_f32(
            h_all, abuf[:, b, 1].reshape(n * cap, quarter), ((0,), (0,))
        ).astype(BF)

    give_back(4)
    give_back(1)

    landed("SHARE", 0, srecv.at[0 : planes - 1])
    sums = srecv[0].astype(F32)
    for j in range(1, planes):
        sums = sums + srecv[j].astype(F32)
    osh_ref[...] = sums

    landed("RG", 0, gret.at[0, 0 : n - 1])
    pieces = []
    for e in range(n):
        full = jnp.broadcast_to(gret[e, 0:1], (8, both_rows))
        row = jnp.where(at_zero, full[:, 0:cap], full[:, cap:both_rows]).astype(BF)
        pieces.append(dot_f32(row, perm[e], ((1,), (0,)))[0:1, :])
    pieces.append(jnp.zeros((128 - n, tok_rows), F32))
    values = jnp.concatenate(pieces, axis=0)
    for k in range(top):
        hit = rtv[k : k + 1, :] == names
        ow_ref[k : k + 1, :] = jnp.sum(jnp.where(hit, values, 0.0), axis=0, keepdims=True)

    landed("RE", 0, ret.at[0 : n - 1])
    otok_ref[...] = dot_f32(
        perm[...].reshape(n * cap, tok_rows), ret[...].reshape(n * cap, quarter), ((0,), (0,))
    ).astype(BF)

    @pl.when(inner)
    def _():
        left(S_ZO, zbuf.at[0:2])
        left(S_TO, tiles.at[0:2])
        left(S_ZR, zbuf.at[0 : planes - 1])
        left(S_TR, tiles.at[0 : planes - 1])

    @pl.when(outer)
    def _():
        left(S_ZO, zbuf.at[0:1])
        left(S_TO, tiles.at[0:1])

    left(S_Y, ysend)
    left(S_YW, wysend)
    left(S_FX, zbuf.at[0 : planes - 1])
    left(S_C0, abuf.at[0, 0:2, :, 0:cap])
    left(S_C, abuf.at[0 : planes - 1, 0:2])
    left(S_RC, crecv)
    left(S_RX, xsend)
    left(S_GC, gpart.at[0, 0 : planes + 1])
    left(S_GX, gtwo.at[0, 0 : planes + 1])
    left(S_RE, ret.at[0 : n - 1])
    left(S_RG, gret.at[0, 0 : n - 1])
    left(S_SHARE, srecv.at[0 : planes - 1])
    left(S_PAIR, spair)


def pass_on(*refs):
    count = len(refs) // 2
    stores = [
        pltpu.make_async_copy(refs[i], refs[count + i], refs[-1].at[i]) for i in range(count)
    ]
    for store in stores:
        store.start()
    for store in stores:
        store.wait()


def hand_over(arrays):
    count = len(arrays)
    return pl.pallas_call(
        pass_on,
        out_shape=tuple(jax.ShapeDtypeStruct(a.shape, a.dtype) for a in arrays),
        in_specs=[pl.BlockSpec(memory_space=pltpu.VMEM)] * count,
        out_specs=tuple([pl.BlockSpec(memory_space=pl.ANY)] * count),
        scratch_shapes=[pltpu.SemaphoreType.DMA((count,))],
    )(*(pltpu.with_memory_space_constraint(a, pltpu.VMEM) for a in arrays))


def fused_shards(
    tokens,
    cotangent,
    route_weights,
    routes,
    gate_proj,
    up_proj,
    down_proj,
    shared_down,
    shared_hidden,
):
    n = lax.axis_size("ep")
    tok_rows, feat = tokens.shape
    top = routes.shape[1]
    units = gate_proj.shape[2]
    hid = shared_hidden.shape[1]
    cap = 2 * tok_rows * top // n
    quarter = feat // 4
    planes = n // 2
    out_shape = (
        pltpu.VMEM((tok_rows, quarter), BF),
        pltpu.VMEM((top, tok_rows), F32),
        pltpu.VMEM((feat, units), BF),
        pltpu.VMEM((feat, units), BF),
        pltpu.VMEM((units, feat), BF),
        pltpu.VMEM((tok_rows, hid), BF),
        pltpu.VMEM((feat // n, hid), F32),
    )
    vmem = pl.BlockSpec(memory_space=pltpu.VMEM)
    hbm = pl.BlockSpec(memory_space=pl.ANY)
    per_piece = pltpu.VMEM((planes + 1, 8, 128), F32)
    outs = pl.pallas_call(
        functools.partial(kernel, n, cap),
        out_shape=out_shape,
        in_specs=[hbm] * 9,
        out_specs=(vmem,) * 7,
        scratch_shapes=[
            pltpu.VMEM((2, tok_rows, feat), BF),
            pltpu.VMEM((top, tok_rows), F32),
            pltpu.VMEM((top, tok_rows), jnp.int32),
            pltpu.VMEM((tok_rows, hid), BF),
            pltpu.VMEM((planes, 2, tok_rows, quarter), BF),
            pltpu.VMEM((planes, 8, tok_rows), F32),
            pltpu.VMEM((planes, 2 * cap, tok_rows), BF),
            pltpu.VMEM((n, cap, tok_rows), BF),
            pltpu.VMEM((planes + 1, 2, cap, quarter), BF),
            pltpu.VMEM((planes, 8, 2 * cap), F32),
            pltpu.VMEM((n, 8, 2 * cap), F32),
            pltpu.VMEM((planes, 4, 2, 2 * cap, quarter), BF),
            pltpu.VMEM((feat, 2 * units), BF),
            pltpu.VMEM((units, feat), BF),
            pltpu.VMEM((feat, hid), BF),
            pltpu.VMEM((planes, 2 * cap, units), BF),
            pltpu.VMEM((planes, 2 * cap, 2 * units), BF),
            pltpu.VMEM((planes, 2, 2, 2 * cap, quarter), BF),
            pltpu.VMEM((planes, 2, 2 * cap, quarter), BF),
            pltpu.VMEM((planes, 2 * cap, quarter), F32),
            pltpu.VMEM((planes, 2 * cap, quarter), BF),
            pltpu.VMEM((planes, 2 * cap, quarter), BF),
            pltpu.VMEM((planes, 2 * cap, quarter), BF),
            pltpu.VMEM((n, cap, quarter), BF),
            per_piece,
            per_piece,
            per_piece,
            per_piece,
            per_piece,
            pltpu.VMEM((n, 8, 128), F32),
            pltpu.VMEM((2, planes, feat // n, hid), BF),
            pltpu.VMEM((planes, feat // n, hid), BF),
            pltpu.VMEM((planes, feat // n, hid), BF),
            pltpu.VMEM((planes, feat // n, hid), BF),
            pltpu.SemaphoreType.DMA((SENDS,)),
            pltpu.SemaphoreType.DMA((ARRIVALS,)),
            pltpu.SemaphoreType.DMA((9,)),
        ],
        compiler_params=pltpu.CompilerParams(
            collective_id=0, has_side_effects=True, vmem_limit_bytes=48 * 1024 * 1024
        ),
    )(
        *(
            pltpu.with_memory_space_constraint(a, pltpu.HBM)
            for a in (
                tokens,
                cotangent,
                route_weights.T,
                routes.T,
                gate_proj[0],
                up_proj[0],
                down_proj[0],
                shared_down,
                shared_hidden,
            )
        )
    )
    outs = hand_over(outs)
    return outs[0], outs[1].T, outs[2][None], outs[3][None], outs[4][None], outs[5], outs[6]


def shards(*args):
    tokens, routes, gate_proj = args[0], args[3], args[4]
    n = lax.axis_size("ep")
    tok_rows, feat = tokens.shape
    top = routes.shape[1]
    fits = (
        gate_proj.shape[0] == 1
        and lax.axis_size("tp") == 4
        and n == 8
        and tok_rows == 128
        and 4 * tok_rows * top == n * tok_rows
        and 2 * top <= 8
        and feat % 512 == 0
        and feat // n % 128 == 0
    )
    if fits:
        return fused_shards(*args)
    return plain_shards(*args)


def plain_shards(
    tokens,
    cotangent,
    route_weights,
    routes,
    gate_proj,
    up_proj,
    down_proj,
    shared_down,
    shared_hidden,
):
    tok_rows, feat_width = tokens.shape
    top_count = routes.shape[1]
    exp_local = gate_proj.shape[0]
    ep_size = lax.axis_size("ep")
    tp_size = lax.axis_size("tp")
    exp_total = exp_local * ep_size
    capacity = 2 * tok_rows * top_count // exp_total
    quarter = feat_width // tp_size
    filled = exp_total * capacity
    flat_routes = routes.reshape(-1)
    one_hot = (flat_routes[:, None] == jnp.arange(exp_total, dtype=jnp.int32)[None, :]).astype(
        jnp.int32
    )
    rank_in = jnp.sum((jnp.cumsum(one_hot, axis=0) - one_hot) * one_hot, axis=1)
    slot_ids = flat_routes * capacity + rank_in
    route_owner = jnp.arange(flat_routes.shape[0], dtype=jnp.int32) // top_count
    owner_ids = jnp.full((filled,), tok_rows, jnp.int32).at[slot_ids].set(route_owner)
    sent_weights = (
        jnp.zeros((filled,), jnp.bfloat16)
        .at[slot_ids]
        .set(route_weights.reshape(-1).astype(jnp.bfloat16))
    )
    first_col = lax.axis_index("tp") * quarter
    own_rows = lax.dynamic_slice_in_dim(tokens, first_col, quarter, 1)
    own_grads = lax.dynamic_slice_in_dim(cotangent, first_col, quarter, 1)
    sent_rows = jnp.take(own_rows, owner_ids, axis=0, mode="fill", fill_value=0)
    sent_grads = jnp.take(own_grads, owner_ids, axis=0, mode="fill", fill_value=0)
    got_rows, got_grads, got_weights = (
        lax.all_to_all(sent_rows, "ep", split_axis=0, concat_axis=0, tiled=True),
        lax.all_to_all(sent_grads, "ep", split_axis=0, concat_axis=0, tiled=True),
        lax.all_to_all(sent_weights, "ep", split_axis=0, concat_axis=0, tiled=True),
    )
    got_rows, got_grads = (
        lax.all_gather(got_rows, "tp", axis=1, tiled=True),
        lax.all_gather(got_grads, "tp", axis=1, tiled=True),
    )
    slot_rows = got_rows.reshape(ep_size, exp_local, capacity, feat_width)
    slot_grads = got_grads.reshape(ep_size, exp_local, capacity, feat_width)
    weight_col = got_weights.reshape(ep_size, exp_local, capacity, 1).astype(jnp.float32)
    gate = jnp.einsum("secd,edf->secf", slot_rows, gate_proj, preferred_element_type=jnp.float32)
    upper = jnp.einsum("secd,edf->secf", slot_rows, up_proj, preferred_element_type=jnp.float32)
    active = jax.nn.silu(gate)
    hidden = (active * upper).astype(jnp.bfloat16)
    backed = jnp.einsum("secd,efd->secf", slot_grads, down_proj, preferred_element_type=jnp.float32)
    gate_share = jnp.sum(hidden.astype(jnp.float32) * backed, axis=3)
    d_hidden = weight_col * backed
    sigma = jax.nn.sigmoid(gate)
    d_gate = (d_hidden * upper * sigma * (1.0 + gate * (1.0 - sigma))).astype(jnp.bfloat16)
    d_up = (d_hidden * active).astype(jnp.bfloat16)
    scaled = (weight_col * slot_grads).astype(jnp.bfloat16)
    down_proj_grad = jnp.einsum(
        "secf,secd->efd", hidden, scaled, preferred_element_type=jnp.float32
    ).astype(jnp.bfloat16)
    gate_proj_grad = jnp.einsum(
        "secd,secf->edf", slot_rows, d_gate, preferred_element_type=jnp.float32
    ).astype(jnp.bfloat16)
    up_proj_grad = jnp.einsum(
        "secd,secf->edf", slot_rows, d_up, preferred_element_type=jnp.float32
    ).astype(jnp.bfloat16)
    partial_value = jnp.einsum(
        "secf,edf->secd", d_gate, gate_proj, preferred_element_type=jnp.float32
    )
    partial_value = partial_value + jnp.einsum(
        "secf,edf->secd", d_up, up_proj, preferred_element_type=jnp.float32
    )
    gate_whole = lax.psum(gate_share, "tp")
    input_cols = lax.psum_scatter(
        partial_value.astype(jnp.bfloat16), "tp", scatter_dimension=3, tiled=True
    )
    back_cols, back_gate = (
        lax.all_to_all(
            input_cols.reshape(filled, quarter), "ep", split_axis=0, concat_axis=0, tiled=True
        ),
        lax.all_to_all(
            gate_whole.astype(jnp.bfloat16).reshape(filled),
            "ep",
            split_axis=0,
            concat_axis=0,
            tiled=True,
        ),
    )
    picked = back_cols[slot_ids].reshape(tok_rows, top_count, quarter)
    tokens_grad = jnp.sum(picked.astype(jnp.float32), axis=1).astype(jnp.bfloat16)
    weights_grad = back_gate[slot_ids].astype(jnp.float32).reshape(tok_rows, top_count)
    hidden_grad = jnp.dot(cotangent, shared_down, preferred_element_type=jnp.float32).astype(
        jnp.bfloat16
    )
    shared_grad = lax.psum_scatter(
        jnp.einsum("td,th->dh", cotangent, shared_hidden, preferred_element_type=jnp.float32),
        "ep",
        scatter_dimension=0,
        tiled=True,
    )
    return (
        tokens_grad,
        weights_grad,
        gate_proj_grad,
        up_proj_grad,
        down_proj_grad,
        hidden_grad,
        shared_grad,
    )


def solution(mesh):
    in_specs = (
        P("ep", None),
        P("ep", None),
        P("ep", None),
        P("ep", None),
        P("ep", None, "tp"),
        P("ep", None, "tp"),
        P("ep", "tp", None),
        P(None, "tp"),
        P("ep", "tp"),
    )
    out_specs = (
        P("ep", "tp"),
        P("ep", None),
        P("ep", None, "tp"),
        P("ep", None, "tp"),
        P("ep", "tp", None),
        P("ep", "tp"),
        P("ep", "tp"),
    )
    return jax.shard_map(shards, mesh=mesh, in_specs=in_specs, out_specs=out_specs, check_vma=False)
```

```python
import functools

import jax
import jax.numpy as jnp
from jax import lax
from jax.experimental import pallas as pl
from jax.experimental.pallas import tpu as pltpu
from jax.sharding import PartitionSpec as P

MESH = pl.DeviceIdType.MESH
BF = jnp.bfloat16
F32 = jnp.float32
S_ZO, S_ZR, S_TO, S_TR, S_Y, S_YW, S_FX, S_C0, S_C = range(9)
S_RC, S_RX, S_GC, S_GX, S_RE, S_RG, S_SHARE, S_PAIR, SENDS = range(9, 18)
COUNTS = {
    "ZF": 16,
    "ZT": 4,
    "Y0": 1,
    "YF": 12,
    "YW": 4,
    "FX": 12,
    "CORE": 4,
    "RC": 10,
    "RX": 7,
    "GC": 5,
    "GX": 5,
    "RE": 1,
    "RG": 1,
    "SHARE": 1,
    "PAIR": 1,
}
FIRST = {kind: sum(list(COUNTS.values())[:i]) for i, kind in enumerate(COUNTS)}
ARRIVALS = sum(COUNTS.values())


def dot_f32(a, b, dims):
    return lax.dot_general(a, b, (dims, ((), ())), preferred_element_type=F32)


def kernel(
    n,
    cap,
    tok_ref,
    cot_ref,
    rw_ref,
    rt_ref,
    wg_ref,
    wu_ref,
    wd_ref,
    sd_ref,
    sh_ref,
    otok_ref,
    ow_ref,
    og_ref,
    ou_ref,
    od_ref,
    ohid_ref,
    osh_ref,
    xg,
    rwv,
    rtv,
    shv,
    zbuf,
    tiles,
    cperm,
    perm,
    ysend,
    wysend,
    wrecv,
    abuf,
    wgu,
    wdv,
    sdv,
    hw,
    dgu,
    part,
    crecv,
    keep,
    xsend,
    xrecv,
    rsend,
    ret,
    gpart,
    gcore,
    gtwo,
    gx,
    gsend,
    gret,
    ssend,
    spair,
    ssum,
    srecv,
    send_sem,
    recv_sem,
    load_sem,
):
    me = lax.axis_index("ep")
    tp = lax.axis_index("tp")
    tok_rows, feat = tok_ref.shape
    top = rt_ref.shape[0]
    quarter = feat // 4
    units = wg_ref.shape[1]
    planes = n // 2
    both_rows = 2 * cap
    y = lax.rem(me, 2)
    z = me // 2
    core_of = lax.rem(tp, 2)
    half_of = tp // 2
    tp_c = half_of * 2 + (1 - core_of)
    tp_x = (1 - half_of) * 2 + core_of
    tp_xc = (1 - half_of) * 2 + (1 - core_of)
    me_y = jnp.bitwise_xor(me, 1)
    inner = (z > 0) & (z < planes - 1)
    outer = (z == 0) | (z == planes - 1)
    low_inner = z == 1
    high_inner = z == planes - 2
    first = jnp.where(z == 0, 1, z - 1)
    second = jnp.where(z == 0, 2, jnp.where(low_inner, z + 1, 0))
    source = [z, first, second, jnp.where(z == planes - 1, 1, planes - 1)]
    pieces_of = range(4)
    part_cols = quarter // 2

    def copy(out, kind, at, src_ref, dst_ref, ep_to, tp_to):
        return pltpu.make_async_remote_copy(
            src_ref=src_ref,
            dst_ref=dst_ref,
            send_sem=send_sem.at[out],
            recv_sem=recv_sem.at[FIRST[kind] + at],
            device_id=(ep_to, tp_to),
            device_id_type=MESH,
        )

    def landed(kind, at, whole_ref):
        copy(0, kind, at, whole_ref, whole_ref, me_y, tp).wait_recv()

    def left(out, whole_ref):
        copy(out, "ZT", 0, whole_ref, whole_ref, me_y, tp).wait_send()

    def rows(block_y):
        return pl.ds(pl.multiple_of(block_y * cap, cap), cap)

    def split(c):
        return c // 2, pl.ds((c % 2) * part_cols, part_cols)

    def columns(block):
        return pl.ds(pl.multiple_of(block * quarter, quarter), quarter)

    barrier = pltpu.get_barrier_semaphore()
    for to in ((me_y, tp), (me, tp_c), (me, tp_x)):
        pl.semaphore_signal(barrier, inc=1, device_id=to, device_id_type=MESH)

    @pl.when(z > 0)
    def _():
        pl.semaphore_signal(barrier, inc=1, device_id=(me - 2, tp), device_id_type=MESH)

    @pl.when(z < planes - 1)
    def _():
        pl.semaphore_signal(barrier, inc=1, device_id=(me + 2, tp), device_id_type=MESH)

    loads = [
        pltpu.make_async_copy(src, dst, load_sem.at[i])
        for i, (src, dst) in enumerate(
            (
                (rt_ref, rtv),
                (rw_ref, rwv),
                (tok_ref, xg.at[0]),
                (cot_ref, xg.at[1]),
                (wg_ref, wgu.at[:, pl.ds(0, units)]),
                (wu_ref, wgu.at[:, pl.ds(units, units)]),
                (wd_ref, wdv),
                (sd_ref, sdv),
                (sh_ref, shv),
            )
        )
    ]
    for load in loads[0:4]:
        load.start()

    before = jnp.where(
        lax.broadcasted_iota(jnp.int32, (tok_rows, tok_rows), 0)
        < lax.broadcasted_iota(jnp.int32, (tok_rows, tok_rows), 1),
        1.0,
        0.0,
    ).astype(BF)
    slot = lax.broadcasted_iota(jnp.int32, (cap, tok_rows), 0).astype(F32)
    two = jnp.where(
        lax.broadcasted_iota(jnp.int32, (8, tok_rows), 0) == 0,
        me.astype(F32),
        me_y.astype(F32),
    )
    at_zero = y == 0

    def place(values):
        low = jnp.where(at_zero, values, 0.0)
        return jnp.concatenate([low, values - low], axis=1)

    def read_tile(i):
        s = source[i]
        named = jnp.zeros((8, tok_rows), F32)
        weight = jnp.zeros((8, tok_rows), F32)
        for k in range(top):
            hit = tiles[s, k : k + 1, :] == two
            named = named + jnp.where(hit, 1.0, 0.0)
            weight = weight + jnp.where(hit, tiles[s, top + k : top + k + 1, :], 0.0)
        rank = dot_f32(named.astype(BF), before, ((1,), (0,)))
        picks = jnp.concatenate(
            [
                jnp.where(slot == rank[j : j + 1, :], named[j : j + 1, :], 0.0).astype(BF)
                for j in range(2)
            ],
            axis=0,
        )
        cperm[i] = picks
        slotted = dot_f32(weight.astype(BF), picks, ((1,), (1,)))
        wrecv[2 * s + y] = jnp.broadcast_to(place(slotted[0:1, 0:cap]), (8, both_rows))
        wysend[i] = jnp.broadcast_to(place(slotted[1:2, cap:both_rows]), (8, both_rows))
        copy(S_YW, "YW", i, wysend.at[i], wrecv.at[2 * s + y], me_y, tp).start()

    def yw_in(i):
        at = 2 * source[i] + (1 - y)
        return copy(S_YW, "YW", i, wrecv.at[at], wrecv.at[at], me_y, tp)

    def yf(i, c):
        p, at = split(c)
        dst = abuf.at[source[i], tp, p, rows(y), at]
        return copy(S_Y, "YF", 4 * (i - 1) + c, ysend.at[i, p, :, at], dst, me_y, tp)

    def y_own(c, block):
        p, at = split(c)
        src = ysend.at[planes if block is tp_x else 0, p, :, at]
        return copy(S_Y, "Y0", 0, src, abuf.at[z, block, p, rows(y), at], me_y, tp)


    def z_own(up, c):
        to = me + 2 if up else me - 2
        p, at = split(c)
        first = pl.multiple_of(tp * quarter + (c % 2) * part_cols, part_cols)
        src = xg.at[p, :, pl.ds(first, part_cols)]
        return copy(S_ZO, "ZF", 4 * z + c, src, zbuf.at[z, p, :, at], to, tp)

    def zt_own(up):
        to = me + 2 if up else me - 2
        return copy(S_TO, "ZT", z, tiles.at[z], tiles.at[z], to, tp)

    def z_relay(i, c):
        s = source[i]
        to = jnp.where(s < z, me + 2, me - 2)
        p, at = split(c)
        block = zbuf.at[s, p, :, at]
        return copy(S_ZR, "ZF", 4 * s + c, block, block, to, tp)

    def zt_relay(i):
        s = source[i]
        to = jnp.where(s < z, me + 2, me - 2)
        return copy(S_TR, "ZT", s, tiles.at[s], tiles.at[s], to, tp)

    def fx(i, j, c):
        block_y = y if j == 0 else 1 - y
        p, at = split(c)
        block = abuf.at[source[i], tp, p, rows(block_y), at]
        return copy(S_FX, "FX", 4 * (i - 1) + c, block, block, me, tp_x)

    def own_to_core(p, block):
        at = abuf.at[z, block, p, rows(1 - y)]
        return copy(S_C0, "CORE", 0, at, at, me, tp_c)

    def to_core(i, c, block):
        p, at = split(c)
        part_of = abuf.at[source[i], block, p, :, at]
        return copy(S_C, "CORE", i, part_of, part_of, me, tp_c)

    rows_each = feat // n

    def pair(q):
        at = pl.ds((q % 2) * (rows_each // 2), rows_each // 2)
        src = ssend.at[1 - y, q // 2, at]
        return copy(S_PAIR, "PAIR", 0, src, spair.at[q // 2, at], me_y, tp)

    def share(d):
        to = jnp.bitwise_xor(z, d)
        return copy(S_SHARE, "SHARE", 0, ssum.at[to], srecv.at[z], 2 * to + y, tp)

    def piece(i):
        if i == 0:
            return z, rows(y), cap
        if i == 1:
            return z, rows(1 - y), cap
        return source[i - 1], pl.ds(0, both_rows), both_rows

    def rc(i, kept):
        s, at, _ = piece(i)
        h = half_of if kept else 1 - half_of
        src = part.at[s, 1 - core_of, h, at]
        return copy(S_RC, "RC", 2 * i + kept, src, crecv.at[s, h, at], me, tp_c)

    def halves(i):
        return ((0, rows(0)), (1, rows(1))) if i >= planes - 1 else ((0, piece(i)[1]),)

    def rx(i, j, at):
        s = piece(i)[0]
        at_sem = i + j + (1 if i == planes else 0)
        return copy(S_RX, "RX", at_sem, xsend.at[s, at], xrecv.at[s, at], me, tp_x)

    def gc(i):
        return copy(S_GC, "GC", i, gpart.at[i, 0:1], gcore.at[i, 0:1], me, tp_c)

    def gxc(i):
        return copy(S_GX, "GX", i, gtwo.at[i, 0:1], gx.at[i, 0:1], me, tp_x)

    def back(i, block_y):
        s = source[i]
        src = rsend.at[s, rows(block_y)]
        return copy(S_RE, "RE", 0, src, ret.at[me], 2 * s + block_y, tp)

    def back_g(i, block_y):
        to = 2 * source[i] + block_y
        return copy(S_RG, "RG", 0, gsend.at[i + 1, 0:1], gret.at[me, 0:1], to, tp)

    def take(i, c, gate=None):
        def run():
            p, at = split(c)
            landed("ZF", 4 * source[i] + c, zbuf.at[source[i], p, :, at])

            @pl.when(low_inner if i == 1 and c > 1 else inner)
            def _():
                z_relay(i, c).start()

        if gate is None:
            run()
        else:
            pl.when(gate)(run)

    def spread(i, c):
        p, at = split(c)
        moved = dot_f32(cperm[i], zbuf[source[i], p, :, at], ((1,), (0,))).astype(BF)
        abuf[source[i], tp, p, rows(y), at] = moved[0:cap]
        ysend[i, p, :, at] = moved[cap:both_rows]
        yf(i, c).start()
        fx(i, 0, c).start()

    def crossed(i, c):
        p, at = split(c)
        landed("YF", 4 * (i - 1) + c, abuf.at[source[i], tp, p, rows(1 - y), at])
        fx(i, 1, c).start()
        to_core(i, c, tp).start()

    def ready(i):
        yw_in(i).wait_recv()
        if i == 0:
            landed("CORE", 0, abuf.at[z, 0:2, :, rows(1 - y)])
        else:
            landed("CORE", i, abuf.at[source[i], 0:2])

    def joined(i, c):
        p, at = split(c)
        landed("FX", 4 * (i - 1) + c, abuf.at[source[i], tp_x, p, :, at])
        to_core(i, c, tp_x).start()

    def compute(i):
        s, at, m = piece(i)
        both = jnp.zeros((m, 2 * units), F32)
        backed = jnp.zeros((m, units), F32)
        for b in range(4):
            cols = slice(b * quarter, (b + 1) * quarter)
            both = both + dot_f32(abuf[s, b, 0, at], wgu[cols, :], ((1,), (0,)))
            backed = backed + dot_f32(abuf[s, b, 1, at], wdv[:, cols], ((1,), (1,)))
        gate = both[:, 0:units]
        upper = both[:, units : 2 * units]
        sigma = jax.nn.sigmoid(gate)
        active = gate * sigma
        hidden = (active * upper).astype(BF).astype(F32)
        if i == 0:
            wrow, first = wrecv[me, 0:1, :], y * cap
        elif i == 1:
            wrow, first = wrecv[me_y, 0:1, :], (1 - y) * cap
        else:
            wrow, first = wrecv[2 * s, 0:1, :] + wrecv[2 * s + 1, 0:1, :], 0
        eye = (
            lax.broadcasted_iota(jnp.int32, (m, both_rows), 0) + first
            == lax.broadcasted_iota(jnp.int32, (m, both_rows), 1)
        )
        wcol = jnp.sum(jnp.where(eye, wrow, 0.0), axis=1, keepdims=True)
        d_hidden = wcol * backed
        hw[s, at] = (wcol * hidden).astype(BF)
        d_both = jnp.concatenate(
            [
                (d_hidden * upper * sigma * (1.0 + gate * (1.0 - sigma))).astype(BF),
                (d_hidden * active).astype(BF),
            ],
            axis=1,
        )
        dgu[s, at] = d_both
        for b in range(4):
            cols = slice(b * quarter, (b + 1) * quarter)
            part[s, b % 2, b // 2, at] = dot_f32(d_both, wgu[cols, :], ((1,), (1,))).astype(BF)
        rc(i, 0).start()
        rc(i, 1).start()
        sums = lax.dot_general(
            jnp.ones((8, units), F32),
            hidden * backed,
            (((1,), (1,)), ((), ())),
            precision=lax.Precision.HIGHEST,
            preferred_element_type=F32,
        )
        if i == 0:
            sums = place(sums)
        elif i == 1:
            low = jnp.where(at_zero, 0.0, sums)
            sums = jnp.concatenate([low, sums - low], axis=1)
        gpart[i] = sums
        gc(i).start()

    def core_sum(i):
        s, whole, _ = piece(i)
        rc(i, 0).wait_recv()
        for j, at in halves(i):
            xsend[s, at] = (
                part[s, core_of, 1 - half_of, at].astype(F32)
                + crecv[s, 1 - half_of, at].astype(F32)
            ).astype(BF)
            rx(i, j, at).start()
            if j == 0:
                gc(i).wait_recv()
                gtwo[i, 0:1] = gpart[i, 0:1] + gcore[i, 0:1]
                gxc(i).start()
        rc(i, 1).wait_recv()
        keep[s, whole] = part[s, core_of, half_of, whole].astype(F32) + crecv[
            s, half_of, whole
        ].astype(F32)

    def give_back(i):
        s, whole, _ = piece(i)
        for j, at in halves(i):
            rx(i, j, at).wait_recv()
            total = (keep[s, at] + xrecv[s, at].astype(F32)).astype(BF)
            if i == 0:
                ret[me] = total
            else:
                rsend[s, at] = total
            if i == 1:
                back(0, 1 - y).start()
            if i == 2:
                back(1, 0).start()
                back(1, 1).start()
            if i > 2:
                back(i - 1, j).start()
            if j == 0:
                gxc(i).wait_recv()
                summed = gtwo[i, 0:1] + gx[i, 0:1]
                if i == 0:
                    gret[me, 0:1] = summed
                else:
                    gsend[i, 0:1] = summed
                if i == 1:
                    back_g(0, 1 - y).start()
                if i > 1:
                    back_g(i - 1, 0).start()
                    back_g(i - 1, 1).start()

    for load in loads[0:2]:
        load.wait()
    tiles[z] = jnp.concatenate(
        [
            rtv[...].astype(F32),
            rwv[...].astype(BF).astype(F32),
            jnp.zeros((8 - 2 * top, tok_rows), F32),
        ],
        axis=0,
    )
    for load in loads[2:4]:
        load.wait()
    for load in loads[4:9]:
        load.start()
    pl.semaphore_wait(
        barrier, 3 + jnp.where(z > 0, 1, 0) + jnp.where(z < planes - 1, 1, 0)
    )

    for up, there in ((True, z < planes - 1), (False, z > 0)):

        @pl.when(there)
        def _():
            zt_own(up).start()
            for c in pieces_of:
                z_own(up, c).start()

    read_tile(0)
    loads[8].wait()
    for j in range(n):
        ssend[j % 2, j // 2] = dot_f32(
            xg[1, :, j * rows_each : (j + 1) * rows_each], shv[...], ((0,), (0,))
        ).astype(BF)
    for q in range(planes):
        pair(q).start()
    other = cperm[0, cap:both_rows, :]
    for p in range(2):
        ysend[0, p] = dot_f32(other, xg[p, :, columns(tp)], ((1,), (0,))).astype(BF)
        ysend[planes, p] = dot_f32(other, xg[p, :, columns(tp_x)], ((1,), (0,))).astype(BF)
    own = cperm[0, 0:cap, :]
    for b in range(4):
        for p in range(2):
            abuf[z, b, p, rows(y)] = dot_f32(
                own, xg[p, :, b * quarter : (b + 1) * quarter], ((1,), (0,))
            ).astype(BF)
    for load in loads[4:8]:
        load.wait()
    compute(0)

    def tile_in(i):
        landed("ZT", source[i], tiles.at[source[i]])

        @pl.when(inner)
        def _():
            zt_relay(i).start()

    late_second = jnp.logical_not(low_inner)
    tile_in(1)
    pl.when(low_inner)(functools.partial(tile_in, 2))
    pl.when(high_inner)(functools.partial(tile_in, 3))
    read_tile(1)
    ohid_ref[...] = dot_f32(xg[1], sdv[...], ((1,), (0,))).astype(BF)
    core_sum(0)
    for c in pieces_of:
        take(1, c)
        take(2, c, low_inner)
        take(3, c, high_inner)
        spread(1, c)
    for q in range(planes, 2 * planes):
        pair(q).start()
    pl.when(late_second)(functools.partial(tile_in, 2))
    crossed(1, 0)
    read_tile(2)

    @pl.when(outer)
    def _():
        for c in pieces_of[1:]:
            crossed(1, c)

    for c in pieces_of:
        take(2, c, late_second)
        spread(2, c)
        if c < 3:
            pl.when(inner)(functools.partial(crossed, 1, c + 1))

    @pl.when(high_inner)
    def _():
        for c in pieces_of[2:]:
            z_relay(1, c).start()

    @pl.when(low_inner)
    def _():
        tile_in(3)
        take(3, 0)

    joined(1, 0)
    take(3, 1, low_inner)
    joined(1, 1)
    take(3, 2, low_inner)
    crossed(2, 0)
    joined(1, 2)
    take(3, 3, low_inner)
    joined(1, 3)
    crossed(2, 1)

    def open_third():
        pl.when(outer)(functools.partial(tile_in, 3))
        read_tile(3)
        for c in pieces_of[0:2]:
            take(3, c, outer)
            spread(3, c)

    pl.when(z > 0)(open_third)
    crossed(2, 2)
    crossed(2, 3)
    pl.when(z == 0)(open_third)
    for c in pieces_of[2:]:
        take(3, c, outer)
        spread(3, c)
    for c in pieces_of:
        y_own(c, tp).start()
        y_own(c, tp_x).start()
    ready(1)
    compute(2)
    joined(2, 0)
    joined(2, 1)
    crossed(3, 0)
    joined(2, 2)
    crossed(3, 1)
    joined(2, 3)
    crossed(3, 2)
    crossed(3, 3)
    core_sum(2)
    landed("PAIR", 0, spair)
    for q in range(planes):
        ssum[q] = (ssend[y, q].astype(F32) + spair[q].astype(F32)).astype(BF)
    srecv[z] = ssum[z]
    for d in range(1, planes):
        share(d).start()
    ready(2)
    compute(3)
    give_back(0)

    names = lax.broadcasted_iota(jnp.int32, (128, tok_rows), 0)
    named_t = jnp.zeros((128, tok_rows), F32)
    for k in range(top):
        named_t = named_t + jnp.where(rtv[k : k + 1, :] == names, 1.0, 0.0)
    rank_t = dot_f32(named_t.astype(BF), before, ((1,), (0,)))
    for e in range(n):
        perm[e] = jnp.where(slot == rank_t[e : e + 1, :], named_t[e : e + 1, :], 0.0).astype(BF)

    core_sum(3)
    for c in pieces_of:
        joined(3, c)
    ready(3)
    compute(4)
    give_back(2)
    core_sum(4)
    landed("Y0", 0, abuf.at[z, 0:2, :, rows(1 - y)])
    for p in range(2):
        own_to_core(p, tp).start()
        own_to_core(p, tp_x).start()
    give_back(3)
    ready(0)
    compute(1)
    core_sum(1)

    d_all = dgu[...].reshape(n * cap, 2 * units)
    h_all = hw[...].reshape(n * cap, units)
    for b in range(4):
        at = slice(b * quarter, (b + 1) * quarter)
        grad = dot_f32(abuf[:, b, 0].reshape(n * cap, quarter), d_all, ((0,), (0,))).astype(BF)
        og_ref[at, :] = grad[:, 0:units]
        ou_ref[at, :] = grad[:, units : 2 * units]
        od_ref[:, at] = dot_f32(
            h_all, abuf[:, b, 1].reshape(n * cap, quarter), ((0,), (0,))
        ).astype(BF)

    give_back(4)
    give_back(1)

    landed("SHARE", 0, srecv.at[0 : planes - 1])
    sums = srecv[0].astype(F32)
    for j in range(1, planes):
        sums = sums + srecv[j].astype(F32)
    osh_ref[...] = sums

    landed("RG", 0, gret.at[0, 0 : n - 1])
    pieces = []
    for e in range(n):
        full = jnp.broadcast_to(gret[e, 0:1], (8, both_rows))
        row = jnp.where(at_zero, full[:, 0:cap], full[:, cap:both_rows]).astype(BF)
        pieces.append(dot_f32(row, perm[e], ((1,), (0,)))[0:1, :])
    pieces.append(jnp.zeros((128 - n, tok_rows), F32))
    values = jnp.concatenate(pieces, axis=0)
    for k in range(top):
        hit = rtv[k : k + 1, :] == names
        ow_ref[k : k + 1, :] = jnp.sum(jnp.where(hit, values, 0.0), axis=0, keepdims=True)

    landed("RE", 0, ret.at[0 : n - 1])
    otok_ref[...] = dot_f32(
        perm[...].reshape(n * cap, tok_rows), ret[...].reshape(n * cap, quarter), ((0,), (0,))
    ).astype(BF)

    @pl.when(inner)
    def _():
        left(S_ZO, zbuf.at[0:2])
        left(S_TO, tiles.at[0:2])
        left(S_ZR, zbuf.at[0 : planes - 1])
        left(S_TR, tiles.at[0 : planes - 1])

    @pl.when(outer)
    def _():
        left(S_ZO, zbuf.at[0:1])
        left(S_TO, tiles.at[0:1])

    left(S_Y, ysend)
    left(S_YW, wysend)
    left(S_FX, zbuf.at[0 : planes - 1])
    left(S_C0, abuf.at[0, 0:2, :, 0:cap])
    left(S_C, abuf.at[0 : planes - 1, 0:2])
    left(S_RC, crecv)
    left(S_RX, xsend)
    left(S_GC, gpart.at[0, 0 : planes + 1])
    left(S_GX, gtwo.at[0, 0 : planes + 1])
    left(S_RE, ret.at[0 : n - 1])
    left(S_RG, gret.at[0, 0 : n - 1])
    left(S_SHARE, srecv.at[0 : planes - 1])
    left(S_PAIR, spair)


def pass_on(*refs):
    count = len(refs) // 2
    stores = [
        pltpu.make_async_copy(refs[i], refs[count + i], refs[-1].at[i]) for i in range(count)
    ]
    for store in stores:
        store.start()
    for store in stores:
        store.wait()


def hand_over(arrays):
    count = len(arrays)
    return pl.pallas_call(
        pass_on,
        out_shape=tuple(jax.ShapeDtypeStruct(a.shape, a.dtype) for a in arrays),
        in_specs=[pl.BlockSpec(memory_space=pltpu.VMEM)] * count,
        out_specs=tuple([pl.BlockSpec(memory_space=pl.ANY)] * count),
        scratch_shapes=[pltpu.SemaphoreType.DMA((count,))],
    )(*(pltpu.with_memory_space_constraint(a, pltpu.VMEM) for a in arrays))


def fused_shards(
    tokens,
    cotangent,
    route_weights,
    routes,
    gate_proj,
    up_proj,
    down_proj,
    shared_down,
    shared_hidden,
):
    n = lax.axis_size("ep")
    tok_rows, feat = tokens.shape
    top = routes.shape[1]
    units = gate_proj.shape[2]
    hid = shared_hidden.shape[1]
    cap = 2 * tok_rows * top // n
    quarter = feat // 4
    planes = n // 2
    out_shape = (
        pltpu.VMEM((tok_rows, quarter), BF),
        pltpu.VMEM((top, tok_rows), F32),
        pltpu.VMEM((feat, units), BF),
        pltpu.VMEM((feat, units), BF),
        pltpu.VMEM((units, feat), BF),
        pltpu.VMEM((tok_rows, hid), BF),
        pltpu.VMEM((feat // n, hid), F32),
    )
    vmem = pl.BlockSpec(memory_space=pltpu.VMEM)
    hbm = pl.BlockSpec(memory_space=pl.ANY)
    per_piece = pltpu.VMEM((planes + 1, 8, 128), F32)
    outs = pl.pallas_call(
        functools.partial(kernel, n, cap),
        out_shape=out_shape,
        in_specs=[hbm] * 9,
        out_specs=(vmem,) * 7,
        scratch_shapes=[
            pltpu.VMEM((2, tok_rows, feat), BF),
            pltpu.VMEM((top, tok_rows), F32),
            pltpu.VMEM((top, tok_rows), jnp.int32),
            pltpu.VMEM((tok_rows, hid), BF),
            pltpu.VMEM((planes, 2, tok_rows, quarter), BF),
            pltpu.VMEM((planes, 8, tok_rows), F32),
            pltpu.VMEM((planes, 2 * cap, tok_rows), BF),
            pltpu.VMEM((n, cap, tok_rows), BF),
            pltpu.VMEM((planes + 1, 2, cap, quarter), BF),
            pltpu.VMEM((planes, 8, 2 * cap), F32),
            pltpu.VMEM((n, 8, 2 * cap), F32),
            pltpu.VMEM((planes, 4, 2, 2 * cap, quarter), BF),
            pltpu.VMEM((feat, 2 * units), BF),
            pltpu.VMEM((units, feat), BF),
            pltpu.VMEM((feat, hid), BF),
            pltpu.VMEM((planes, 2 * cap, units), BF),
            pltpu.VMEM((planes, 2 * cap, 2 * units), BF),
            pltpu.VMEM((planes, 2, 2, 2 * cap, quarter), BF),
            pltpu.VMEM((planes, 2, 2 * cap, quarter), BF),
            pltpu.VMEM((planes, 2 * cap, quarter), F32),
            pltpu.VMEM((planes, 2 * cap, quarter), BF),
            pltpu.VMEM((planes, 2 * cap, quarter), BF),
            pltpu.VMEM((planes, 2 * cap, quarter), BF),
            pltpu.VMEM((n, cap, quarter), BF),
            per_piece,
            per_piece,
            per_piece,
            per_piece,
            per_piece,
            pltpu.VMEM((n, 8, 128), F32),
            pltpu.VMEM((2, planes, feat // n, hid), BF),
            pltpu.VMEM((planes, feat // n, hid), BF),
            pltpu.VMEM((planes, feat // n, hid), BF),
            pltpu.VMEM((planes, feat // n, hid), BF),
            pltpu.SemaphoreType.DMA((SENDS,)),
            pltpu.SemaphoreType.DMA((ARRIVALS,)),
            pltpu.SemaphoreType.DMA((9,)),
        ],
        compiler_params=pltpu.CompilerParams(
            collective_id=0, has_side_effects=True, vmem_limit_bytes=48 * 1024 * 1024
        ),
    )(
        *(
            pltpu.with_memory_space_constraint(a, pltpu.HBM)
            for a in (
                tokens,
                cotangent,
                route_weights.T,
                routes.T,
                gate_proj[0],
                up_proj[0],
                down_proj[0],
                shared_down,
                shared_hidden,
            )
        )
    )
    outs = hand_over(outs)
    return outs[0], outs[1].T, outs[2][None], outs[3][None], outs[4][None], outs[5], outs[6]


def shards(*args):
    tokens, routes, gate_proj = args[0], args[3], args[4]
    n = lax.axis_size("ep")
    tok_rows, feat = tokens.shape
    top = routes.shape[1]
    fits = (
        gate_proj.shape[0] == 1
        and lax.axis_size("tp") == 4
        and n == 8
        and tok_rows == 128
        and 4 * tok_rows * top == n * tok_rows
        and 2 * top <= 8
        and feat % 512 == 0
        and feat // n % 128 == 0
    )
    if fits:
        return fused_shards(*args)
    return plain_shards(*args)


def plain_shards(
    tokens,
    cotangent,
    route_weights,
    routes,
    gate_proj,
    up_proj,
    down_proj,
    shared_down,
    shared_hidden,
):
    tok_rows, feat_width = tokens.shape
    top_count = routes.shape[1]
    exp_local = gate_proj.shape[0]
    ep_size = lax.axis_size("ep")
    tp_size = lax.axis_size("tp")
    exp_total = exp_local * ep_size
    capacity = 2 * tok_rows * top_count // exp_total
    quarter = feat_width // tp_size
    filled = exp_total * capacity
    flat_routes = routes.reshape(-1)
    one_hot = (flat_routes[:, None] == jnp.arange(exp_total, dtype=jnp.int32)[None, :]).astype(
        jnp.int32
    )
    rank_in = jnp.sum((jnp.cumsum(one_hot, axis=0) - one_hot) * one_hot, axis=1)
    slot_ids = flat_routes * capacity + rank_in
    route_owner = jnp.arange(flat_routes.shape[0], dtype=jnp.int32) // top_count
    owner_ids = jnp.full((filled,), tok_rows, jnp.int32).at[slot_ids].set(route_owner)
    sent_weights = (
        jnp.zeros((filled,), jnp.bfloat16)
        .at[slot_ids]
        .set(route_weights.reshape(-1).astype(jnp.bfloat16))
    )
    first_col = lax.axis_index("tp") * quarter
    own_rows = lax.dynamic_slice_in_dim(tokens, first_col, quarter, 1)
    own_grads = lax.dynamic_slice_in_dim(cotangent, first_col, quarter, 1)
    sent_rows = jnp.take(own_rows, owner_ids, axis=0, mode="fill", fill_value=0)
    sent_grads = jnp.take(own_grads, owner_ids, axis=0, mode="fill", fill_value=0)
    got_rows, got_grads, got_weights = (
        lax.all_to_all(sent_rows, "ep", split_axis=0, concat_axis=0, tiled=True),
        lax.all_to_all(sent_grads, "ep", split_axis=0, concat_axis=0, tiled=True),
        lax.all_to_all(sent_weights, "ep", split_axis=0, concat_axis=0, tiled=True),
    )
    got_rows, got_grads = (
        lax.all_gather(got_rows, "tp", axis=1, tiled=True),
        lax.all_gather(got_grads, "tp", axis=1, tiled=True),
    )
    slot_rows = got_rows.reshape(ep_size, exp_local, capacity, feat_width)
    slot_grads = got_grads.reshape(ep_size, exp_local, capacity, feat_width)
    weight_col = got_weights.reshape(ep_size, exp_local, capacity, 1).astype(jnp.float32)
    gate = jnp.einsum("secd,edf->secf", slot_rows, gate_proj, preferred_element_type=jnp.float32)
    upper = jnp.einsum("secd,edf->secf", slot_rows, up_proj, preferred_element_type=jnp.float32)
    active = jax.nn.silu(gate)
    hidden = (active * upper).astype(jnp.bfloat16)
    backed = jnp.einsum("secd,efd->secf", slot_grads, down_proj, preferred_element_type=jnp.float32)
    gate_share = jnp.sum(hidden.astype(jnp.float32) * backed, axis=3)
    d_hidden = weight_col * backed
    sigma = jax.nn.sigmoid(gate)
    d_gate = (d_hidden * upper * sigma * (1.0 + gate * (1.0 - sigma))).astype(jnp.bfloat16)
    d_up = (d_hidden * active).astype(jnp.bfloat16)
    scaled = (weight_col * slot_grads).astype(jnp.bfloat16)
    down_proj_grad = jnp.einsum(
        "secf,secd->efd", hidden, scaled, preferred_element_type=jnp.float32
    ).astype(jnp.bfloat16)
    gate_proj_grad = jnp.einsum(
        "secd,secf->edf", slot_rows, d_gate, preferred_element_type=jnp.float32
    ).astype(jnp.bfloat16)
    up_proj_grad = jnp.einsum(
        "secd,secf->edf", slot_rows, d_up, preferred_element_type=jnp.float32
    ).astype(jnp.bfloat16)
    partial_value = jnp.einsum(
        "secf,edf->secd", d_gate, gate_proj, preferred_element_type=jnp.float32
    )
    partial_value = partial_value + jnp.einsum(
        "secf,edf->secd", d_up, up_proj, preferred_element_type=jnp.float32
    )
    gate_whole = lax.psum(gate_share, "tp")
    input_cols = lax.psum_scatter(
        partial_value.astype(jnp.bfloat16), "tp", scatter_dimension=3, tiled=True
    )
    back_cols, back_gate = (
        lax.all_to_all(
            input_cols.reshape(filled, quarter), "ep", split_axis=0, concat_axis=0, tiled=True
        ),
        lax.all_to_all(
            gate_whole.astype(jnp.bfloat16).reshape(filled),
            "ep",
            split_axis=0,
            concat_axis=0,
            tiled=True,
        ),
    )
    picked = back_cols[slot_ids].reshape(tok_rows, top_count, quarter)
    tokens_grad = jnp.sum(picked.astype(jnp.float32), axis=1).astype(jnp.bfloat16)
    weights_grad = back_gate[slot_ids].astype(jnp.float32).reshape(tok_rows, top_count)
    hidden_grad = jnp.dot(cotangent, shared_down, preferred_element_type=jnp.float32).astype(
        jnp.bfloat16
    )
    shared_grad = lax.psum_scatter(
        jnp.einsum("td,th->dh", cotangent, shared_hidden, preferred_element_type=jnp.float32),
        "ep",
        scatter_dimension=0,
        tiled=True,
    )
    return (
        tokens_grad,
        weights_grad,
        gate_proj_grad,
        up_proj_grad,
        down_proj_grad,
        hidden_grad,
        shared_grad,
    )


def solution(mesh):
    in_specs = (
        P("ep", None),
        P("ep", None),
        P("ep", None),
        P("ep", None),
        P("ep", None, "tp"),
        P("ep", None, "tp"),
        P("ep", "tp", None),
        P(None, "tp"),
        P("ep", "tp"),
    )
    out_specs = (
        P("ep", "tp"),
        P("ep", None),
        P("ep", None, "tp"),
        P("ep", None, "tp"),
        P("ep", "tp", None),
        P("ep", "tp"),
        P("ep", "tp"),
    )
    return jax.shard_map(shards, mesh=mesh, in_specs=in_specs, out_specs=out_specs, check_vma=False)
```

```python
import functools

import jax
import jax.numpy as jnp
from jax import lax
from jax.experimental import pallas as pl
from jax.experimental.pallas import tpu as pltpu
from jax.sharding import PartitionSpec as P

MESH = pl.DeviceIdType.MESH
BF = jnp.bfloat16
F32 = jnp.float32
S_ZO, S_ZR, S_TO, S_TR, S_Y, S_YW, S_FX, S_C0, S_C = range(9)
S_RC, S_RX, S_GC, S_GX, S_RE, S_RG, S_SHARE, S_PAIR, SENDS = range(9, 18)
COUNTS = {
    "ZF": 16,
    "ZT": 4,
    "Y0": 1,
    "YF": 12,
    "YW": 4,
    "FX": 12,
    "CORE": 4,
    "RC": 10,
    "RX": 7,
    "GC": 5,
    "GX": 5,
    "RE": 1,
    "RG": 1,
    "SHARE": 1,
    "PAIR": 1,
}
FIRST = {kind: sum(list(COUNTS.values())[:i]) for i, kind in enumerate(COUNTS)}
ARRIVALS = sum(COUNTS.values())


def dot_f32(a, b, dims):
    return lax.dot_general(a, b, (dims, ((), ())), preferred_element_type=F32)


def kernel(
    n,
    cap,
    tok_ref,
    cot_ref,
    rw_ref,
    rt_ref,
    wg_ref,
    wu_ref,
    wd_ref,
    sd_ref,
    sh_ref,
    otok_ref,
    ow_ref,
    og_ref,
    ou_ref,
    od_ref,
    ohid_ref,
    osh_ref,
    xg,
    rwv,
    rtv,
    shv,
    zbuf,
    tiles,
    cperm,
    perm,
    ysend,
    wysend,
    wrecv,
    abuf,
    wgu,
    wdv,
    sdv,
    hw,
    dgu,
    part,
    crecv,
    keep,
    xsend,
    xrecv,
    rsend,
    ret,
    gpart,
    gcore,
    gtwo,
    gx,
    gsend,
    gret,
    ssend,
    spair,
    ssum,
    srecv,
    send_sem,
    recv_sem,
    load_sem,
):
    me = lax.axis_index("ep")
    tp = lax.axis_index("tp")
    tok_rows, feat = tok_ref.shape
    top = rt_ref.shape[0]
    quarter = feat // 4
    units = wg_ref.shape[1]
    planes = n // 2
    both_rows = 2 * cap
    y = lax.rem(me, 2)
    z = me // 2
    core_of = lax.rem(tp, 2)
    half_of = tp // 2
    tp_c = half_of * 2 + (1 - core_of)
    tp_x = (1 - half_of) * 2 + core_of
    tp_xc = (1 - half_of) * 2 + (1 - core_of)
    me_y = jnp.bitwise_xor(me, 1)
    inner = (z > 0) & (z < planes - 1)
    outer = (z == 0) | (z == planes - 1)
    low_inner = z == 1
    high_inner = z == planes - 2
    first = jnp.where(z == 0, 1, z - 1)
    second = jnp.where(z == 0, 2, jnp.where(low_inner, planes - 1, 0))
    third = jnp.where(z == planes - 1, 1, jnp.where(low_inner, 2, planes - 1))
    source = [z, first, second, third]
    pieces_of = range(4)
    part_cols = quarter // 2

    def copy(out, kind, at, src_ref, dst_ref, ep_to, tp_to):
        return pltpu.make_async_remote_copy(
            src_ref=src_ref,
            dst_ref=dst_ref,
            send_sem=send_sem.at[out],
            recv_sem=recv_sem.at[FIRST[kind] + at],
            device_id=(ep_to, tp_to),
            device_id_type=MESH,
        )

    def landed(kind, at, whole_ref):
        copy(0, kind, at, whole_ref, whole_ref, me_y, tp).wait_recv()

    def left(out, whole_ref):
        copy(out, "ZT", 0, whole_ref, whole_ref, me_y, tp).wait_send()

    def rows(block_y):
        return pl.ds(pl.multiple_of(block_y * cap, cap), cap)

    def split(c):
        return c // 2, pl.ds((c % 2) * part_cols, part_cols)

    def columns(block):
        return pl.ds(pl.multiple_of(block * quarter, quarter), quarter)

    barrier = pltpu.get_barrier_semaphore()
    for to in ((me_y, tp), (me, tp_c), (me, tp_x)):
        pl.semaphore_signal(barrier, inc=1, device_id=to, device_id_type=MESH)

    @pl.when(z > 0)
    def _():
        pl.semaphore_signal(barrier, inc=1, device_id=(me - 2, tp), device_id_type=MESH)

    @pl.when(z < planes - 1)
    def _():
        pl.semaphore_signal(barrier, inc=1, device_id=(me + 2, tp), device_id_type=MESH)

    loads = [
        pltpu.make_async_copy(src, dst, load_sem.at[i])
        for i, (src, dst) in enumerate(
            (
                (rt_ref, rtv),
                (rw_ref, rwv),
                (tok_ref, xg.at[0]),
                (cot_ref, xg.at[1]),
                (wg_ref, wgu.at[:, pl.ds(0, units)]),
                (wu_ref, wgu.at[:, pl.ds(units, units)]),
                (wd_ref, wdv),
                (sd_ref, sdv),
                (sh_ref, shv),
            )
        )
    ]
    for load in loads[0:4]:
        load.start()

    before = jnp.where(
        lax.broadcasted_iota(jnp.int32, (tok_rows, tok_rows), 0)
        < lax.broadcasted_iota(jnp.int32, (tok_rows, tok_rows), 1),
        1.0,
        0.0,
    ).astype(BF)
    slot = lax.broadcasted_iota(jnp.int32, (cap, tok_rows), 0).astype(F32)
    two = jnp.where(
        lax.broadcasted_iota(jnp.int32, (8, tok_rows), 0) == 0,
        me.astype(F32),
        me_y.astype(F32),
    )
    at_zero = y == 0

    def place(values):
        low = jnp.where(at_zero, values, 0.0)
        return jnp.concatenate([low, values - low], axis=1)

    def read_tile(i):
        s = source[i]
        named = jnp.zeros((8, tok_rows), F32)
        weight = jnp.zeros((8, tok_rows), F32)
        for k in range(top):
            hit = tiles[s, k : k + 1, :] == two
            named = named + jnp.where(hit, 1.0, 0.0)
            weight = weight + jnp.where(hit, tiles[s, top + k : top + k + 1, :], 0.0)
        rank = dot_f32(named.astype(BF), before, ((1,), (0,)))
        picks = jnp.concatenate(
            [
                jnp.where(slot == rank[j : j + 1, :], named[j : j + 1, :], 0.0).astype(BF)
                for j in range(2)
            ],
            axis=0,
        )
        cperm[i] = picks
        slotted = dot_f32(weight.astype(BF), picks, ((1,), (1,)))
        wrecv[2 * s + y] = jnp.broadcast_to(place(slotted[0:1, 0:cap]), (8, both_rows))
        wysend[i] = jnp.broadcast_to(place(slotted[1:2, cap:both_rows]), (8, both_rows))
        copy(S_YW, "YW", i, wysend.at[i], wrecv.at[2 * s + y], me_y, tp).start()

    def yw_in(i):
        at = 2 * source[i] + (1 - y)
        return copy(S_YW, "YW", i, wrecv.at[at], wrecv.at[at], me_y, tp)

    def yf(i, c):
        p, at = split(c)
        dst = abuf.at[source[i], tp, p, rows(y), at]
        return copy(S_Y, "YF", 4 * (i - 1) + c, ysend.at[i, p, :, at], dst, me_y, tp)

    def y_own(c, block):
        p, at = split(c)
        src = ysend.at[planes if block is tp_x else 0, p, :, at]
        return copy(S_Y, "Y0", 0, src, abuf.at[z, block, p, rows(y), at], me_y, tp)


    def z_own(up, c):
        to = me + 2 if up else me - 2
        p, at = split(c)
        first = pl.multiple_of(tp * quarter + (c % 2) * part_cols, part_cols)
        src = xg.at[p, :, pl.ds(first, part_cols)]
        return copy(S_ZO, "ZF", 4 * z + c, src, zbuf.at[z, p, :, at], to, tp)

    def zt_own(up):
        to = me + 2 if up else me - 2
        return copy(S_TO, "ZT", z, tiles.at[z], tiles.at[z], to, tp)

    def z_relay(i, c):
        s = source[i]
        to = jnp.where(s < z, me + 2, me - 2)
        p, at = split(c)
        block = zbuf.at[s, p, :, at]
        return copy(S_ZR, "ZF", 4 * s + c, block, block, to, tp)

    def zt_relay(i):
        s = source[i]
        to = jnp.where(s < z, me + 2, me - 2)
        return copy(S_TR, "ZT", s, tiles.at[s], tiles.at[s], to, tp)

    def fx(i, j, c):
        block_y = y if j == 0 else 1 - y
        p, at = split(c)
        block = abuf.at[source[i], tp, p, rows(block_y), at]
        return copy(S_FX, "FX", 4 * (i - 1) + c, block, block, me, tp_x)

    def own_to_core(p, block):
        at = abuf.at[z, block, p, rows(1 - y)]
        return copy(S_C0, "CORE", 0, at, at, me, tp_c)

    def to_core(i, c, block):
        p, at = split(c)
        part_of = abuf.at[source[i], block, p, :, at]
        return copy(S_C, "CORE", i, part_of, part_of, me, tp_c)

    rows_each = feat // n

    def pair(q):
        at = pl.ds((q % 2) * (rows_each // 2), rows_each // 2)
        src = ssend.at[1 - y, q // 2, at]
        return copy(S_PAIR, "PAIR", 0, src, spair.at[q // 2, at], me_y, tp)

    def share(d):
        to = jnp.bitwise_xor(z, d)
        return copy(S_SHARE, "SHARE", 0, ssum.at[to], srecv.at[z], 2 * to + y, tp)

    def piece(i):
        if i == 0:
            return z, rows(y), cap
        if i == 1:
            return z, rows(1 - y), cap
        return source[i - 1], pl.ds(0, both_rows), both_rows

    def rc(i, kept):
        s, at, _ = piece(i)
        h = half_of if kept else 1 - half_of
        src = part.at[s, 1 - core_of, h, at]
        return copy(S_RC, "RC", 2 * i + kept, src, crecv.at[s, h, at], me, tp_c)

    def halves(i):
        return ((0, rows(0)), (1, rows(1))) if i >= planes - 1 else ((0, piece(i)[1]),)

    def rx(i, j, at):
        s = piece(i)[0]
        at_sem = i + j + (1 if i == planes else 0)
        return copy(S_RX, "RX", at_sem, xsend.at[s, at], xrecv.at[s, at], me, tp_x)

    def gc(i):
        return copy(S_GC, "GC", i, gpart.at[i, 0:1], gcore.at[i, 0:1], me, tp_c)

    def gxc(i):
        return copy(S_GX, "GX", i, gtwo.at[i, 0:1], gx.at[i, 0:1], me, tp_x)

    def back(i, block_y):
        s = source[i]
        src = rsend.at[s, rows(block_y)]
        return copy(S_RE, "RE", 0, src, ret.at[me], 2 * s + block_y, tp)

    def back_g(i, block_y):
        to = 2 * source[i] + block_y
        return copy(S_RG, "RG", 0, gsend.at[i + 1, 0:1], gret.at[me, 0:1], to, tp)

    def take(i, c, gate=None):
        def run():
            p, at = split(c)
            landed("ZF", 4 * source[i] + c, zbuf.at[source[i], p, :, at])

            @pl.when(low_inner if i == 1 and c > 1 else inner)
            def _():
                z_relay(i, c).start()

        if gate is None:
            run()
        else:
            pl.when(gate)(run)

    def spread(i, c):
        p, at = split(c)
        moved = dot_f32(cperm[i], zbuf[source[i], p, :, at], ((1,), (0,))).astype(BF)
        abuf[source[i], tp, p, rows(y), at] = moved[0:cap]
        ysend[i, p, :, at] = moved[cap:both_rows]
        yf(i, c).start()
        fx(i, 0, c).start()

    def crossed(i, c):
        p, at = split(c)
        landed("YF", 4 * (i - 1) + c, abuf.at[source[i], tp, p, rows(1 - y), at])
        fx(i, 1, c).start()
        to_core(i, c, tp).start()

    def ready(i):
        yw_in(i).wait_recv()
        if i == 0:
            landed("CORE", 0, abuf.at[z, 0:2, :, rows(1 - y)])
        else:
            landed("CORE", i, abuf.at[source[i], 0:2])

    def joined(i, c):
        p, at = split(c)
        landed("FX", 4 * (i - 1) + c, abuf.at[source[i], tp_x, p, :, at])
        to_core(i, c, tp_x).start()

    def compute(i):
        s, at, m = piece(i)
        both = jnp.zeros((m, 2 * units), F32)
        backed = jnp.zeros((m, units), F32)
        for b in range(4):
            cols = slice(b * quarter, (b + 1) * quarter)
            both = both + dot_f32(abuf[s, b, 0, at], wgu[cols, :], ((1,), (0,)))
            backed = backed + dot_f32(abuf[s, b, 1, at], wdv[:, cols], ((1,), (1,)))
        gate = both[:, 0:units]
        upper = both[:, units : 2 * units]
        sigma = jax.nn.sigmoid(gate)
        active = gate * sigma
        hidden = (active * upper).astype(BF).astype(F32)
        if i == 0:
            wrow, first = wrecv[me, 0:1, :], y * cap
        elif i == 1:
            wrow, first = wrecv[me_y, 0:1, :], (1 - y) * cap
        else:
            wrow, first = wrecv[2 * s, 0:1, :] + wrecv[2 * s + 1, 0:1, :], 0
        eye = (
            lax.broadcasted_iota(jnp.int32, (m, both_rows), 0) + first
            == lax.broadcasted_iota(jnp.int32, (m, both_rows), 1)
        )
        wcol = jnp.sum(jnp.where(eye, wrow, 0.0), axis=1, keepdims=True)
        d_hidden = wcol * backed
        hw[s, at] = (wcol * hidden).astype(BF)
        d_both = jnp.concatenate(
            [
                (d_hidden * upper * sigma * (1.0 + gate * (1.0 - sigma))).astype(BF),
                (d_hidden * active).astype(BF),
            ],
            axis=1,
        )
        dgu[s, at] = d_both
        for b in range(4):
            cols = slice(b * quarter, (b + 1) * quarter)
            part[s, b % 2, b // 2, at] = dot_f32(d_both, wgu[cols, :], ((1,), (1,))).astype(BF)
        rc(i, 0).start()
        rc(i, 1).start()
        sums = lax.dot_general(
            jnp.ones((8, units), F32),
            hidden * backed,
            (((1,), (1,)), ((), ())),
            precision=lax.Precision.HIGHEST,
            preferred_element_type=F32,
        )
        if i == 0:
            sums = place(sums)
        elif i == 1:
            low = jnp.where(at_zero, 0.0, sums)
            sums = jnp.concatenate([low, sums - low], axis=1)
        gpart[i] = sums
        gc(i).start()

    def core_sum(i):
        s, whole, _ = piece(i)
        rc(i, 0).wait_recv()
        for j, at in halves(i):
            xsend[s, at] = (
                part[s, core_of, 1 - half_of, at].astype(F32)
                + crecv[s, 1 - half_of, at].astype(F32)
            ).astype(BF)
            rx(i, j, at).start()
            if j == 0:
                gc(i).wait_recv()
                gtwo[i, 0:1] = gpart[i, 0:1] + gcore[i, 0:1]
                gxc(i).start()
        rc(i, 1).wait_recv()
        keep[s, whole] = part[s, core_of, half_of, whole].astype(F32) + crecv[
            s, half_of, whole
        ].astype(F32)

    def give_back(i):
        s, whole, _ = piece(i)
        for j, at in halves(i):
            rx(i, j, at).wait_recv()
            total = (keep[s, at] + xrecv[s, at].astype(F32)).astype(BF)
            if i == 0:
                ret[me] = total
            else:
                rsend[s, at] = total
            if i == 1:
                back(0, 1 - y).start()
            if i == 2:
                back(1, 0).start()
                back(1, 1).start()
            if i > 2:
                back(i - 1, j).start()
            if j == 0:
                gxc(i).wait_recv()
                summed = gtwo[i, 0:1] + gx[i, 0:1]
                if i == 0:
                    gret[me, 0:1] = summed
                else:
                    gsend[i, 0:1] = summed
                if i == 1:
                    back_g(0, 1 - y).start()
                if i > 1:
                    back_g(i - 1, 0).start()
                    back_g(i - 1, 1).start()

    for load in loads[0:2]:
        load.wait()
    tiles[z] = jnp.concatenate(
        [
            rtv[...].astype(F32),
            rwv[...].astype(BF).astype(F32),
            jnp.zeros((8 - 2 * top, tok_rows), F32),
        ],
        axis=0,
    )
    for load in loads[2:4]:
        load.wait()
    for load in loads[4:9]:
        load.start()
    pl.semaphore_wait(
        barrier, 3 + jnp.where(z > 0, 1, 0) + jnp.where(z < planes - 1, 1, 0)
    )

    for up, there in ((True, z < planes - 1), (False, z > 0)):

        @pl.when(there)
        def _():
            zt_own(up).start()
            for c in pieces_of:
                z_own(up, c).start()

    read_tile(0)
    loads[8].wait()
    for j in range(n):
        ssend[j % 2, j // 2] = dot_f32(
            xg[1, :, j * rows_each : (j + 1) * rows_each], shv[...], ((0,), (0,))
        ).astype(BF)
    for q in range(planes):
        pair(q).start()
    other = cperm[0, cap:both_rows, :]
    for p in range(2):
        ysend[0, p] = dot_f32(other, xg[p, :, columns(tp)], ((1,), (0,))).astype(BF)
        ysend[planes, p] = dot_f32(other, xg[p, :, columns(tp_x)], ((1,), (0,))).astype(BF)
    own = cperm[0, 0:cap, :]
    for b in range(4):
        for p in range(2):
            abuf[z, b, p, rows(y)] = dot_f32(
                own, xg[p, :, b * quarter : (b + 1) * quarter], ((1,), (0,))
            ).astype(BF)
    for load in loads[4:8]:
        load.wait()
    compute(0)

    def tile_in(i):
        landed("ZT", source[i], tiles.at[source[i]])

        @pl.when(inner)
        def _():
            zt_relay(i).start()

    tile_in(1)
    pl.when(inner)(functools.partial(tile_in, 3))
    read_tile(1)
    ohid_ref[...] = dot_f32(xg[1], sdv[...], ((1,), (0,))).astype(BF)
    core_sum(0)
    for c in pieces_of:
        take(1, c)
        take(3, c, inner)
        spread(1, c)
    for q in range(planes, 2 * planes):
        pair(q).start()
    tile_in(2)
    crossed(1, 0)
    read_tile(2)

    @pl.when(outer)
    def _():
        for c in pieces_of[1:]:
            crossed(1, c)

    for c in pieces_of:
        take(2, c)
        spread(2, c)
        if c < 3:
            pl.when(inner)(functools.partial(crossed, 1, c + 1))

    @pl.when(high_inner)
    def _():
        for c in pieces_of[2:]:
            z_relay(1, c).start()

    joined(1, 0)
    joined(1, 1)
    crossed(2, 0)
    joined(1, 2)
    joined(1, 3)
    crossed(2, 1)

    def open_third():
        pl.when(outer)(functools.partial(tile_in, 3))
        read_tile(3)
        for c in pieces_of[0:2]:
            take(3, c, outer)
            spread(3, c)

    pl.when(z > 0)(open_third)
    crossed(2, 2)
    crossed(2, 3)
    pl.when(z == 0)(open_third)
    for c in pieces_of[2:]:
        take(3, c, outer)
        spread(3, c)
    for c in pieces_of:
        y_own(c, tp).start()
        y_own(c, tp_x).start()
    ready(1)
    compute(2)
    joined(2, 0)
    joined(2, 1)
    crossed(3, 0)
    joined(2, 2)
    crossed(3, 1)
    joined(2, 3)
    crossed(3, 2)
    crossed(3, 3)
    core_sum(2)
    landed("PAIR", 0, spair)
    for q in range(planes):
        ssum[q] = (ssend[y, q].astype(F32) + spair[q].astype(F32)).astype(BF)
    srecv[z] = ssum[z]
    for d in range(1, planes):
        share(d).start()
    ready(2)
    compute(3)
    give_back(0)

    names = lax.broadcasted_iota(jnp.int32, (128, tok_rows), 0)
    named_t = jnp.zeros((128, tok_rows), F32)
    for k in range(top):
        named_t = named_t + jnp.where(rtv[k : k + 1, :] == names, 1.0, 0.0)
    rank_t = dot_f32(named_t.astype(BF), before, ((1,), (0,)))
    for e in range(n):
        perm[e] = jnp.where(slot == rank_t[e : e + 1, :], named_t[e : e + 1, :], 0.0).astype(BF)

    core_sum(3)
    for c in pieces_of:
        joined(3, c)
    ready(3)
    compute(4)
    give_back(2)
    core_sum(4)
    landed("Y0", 0, abuf.at[z, 0:2, :, rows(1 - y)])
    for p in range(2):
        own_to_core(p, tp).start()
        own_to_core(p, tp_x).start()
    give_back(3)
    ready(0)
    compute(1)
    core_sum(1)

    d_all = dgu[...].reshape(n * cap, 2 * units)
    h_all = hw[...].reshape(n * cap, units)
    for b in range(4):
        at = slice(b * quarter, (b + 1) * quarter)
        grad = dot_f32(abuf[:, b, 0].reshape(n * cap, quarter), d_all, ((0,), (0,))).astype(BF)
        og_ref[at, :] = grad[:, 0:units]
        ou_ref[at, :] = grad[:, units : 2 * units]
        od_ref[:, at] = dot_f32(
            h_all, abuf[:, b, 1].reshape(n * cap, quarter), ((0,), (0,))
        ).astype(BF)

    give_back(4)
    give_back(1)

    landed("SHARE", 0, srecv.at[0 : planes - 1])
    sums = srecv[0].astype(F32)
    for j in range(1, planes):
        sums = sums + srecv[j].astype(F32)
    osh_ref[...] = sums

    landed("RG", 0, gret.at[0, 0 : n - 1])
    pieces = []
    for e in range(n):
        full = jnp.broadcast_to(gret[e, 0:1], (8, both_rows))
        row = jnp.where(at_zero, full[:, 0:cap], full[:, cap:both_rows]).astype(BF)
        pieces.append(dot_f32(row, perm[e], ((1,), (0,)))[0:1, :])
    pieces.append(jnp.zeros((128 - n, tok_rows), F32))
    values = jnp.concatenate(pieces, axis=0)
    for k in range(top):
        hit = rtv[k : k + 1, :] == names
        ow_ref[k : k + 1, :] = jnp.sum(jnp.where(hit, values, 0.0), axis=0, keepdims=True)

    landed("RE", 0, ret.at[0 : n - 1])
    otok_ref[...] = dot_f32(
        perm[...].reshape(n * cap, tok_rows), ret[...].reshape(n * cap, quarter), ((0,), (0,))
    ).astype(BF)

    @pl.when(inner)
    def _():
        left(S_ZO, zbuf.at[0:2])
        left(S_TO, tiles.at[0:2])
        left(S_ZR, zbuf.at[0 : planes - 1])
        left(S_TR, tiles.at[0 : planes - 1])

    @pl.when(outer)
    def _():
        left(S_ZO, zbuf.at[0:1])
        left(S_TO, tiles.at[0:1])

    left(S_Y, ysend)
    left(S_YW, wysend)
    left(S_FX, zbuf.at[0 : planes - 1])
    left(S_C0, abuf.at[0, 0:2, :, 0:cap])
    left(S_C, abuf.at[0 : planes - 1, 0:2])
    left(S_RC, crecv)
    left(S_RX, xsend)
    left(S_GC, gpart.at[0, 0 : planes + 1])
    left(S_GX, gtwo.at[0, 0 : planes + 1])
    left(S_RE, ret.at[0 : n - 1])
    left(S_RG, gret.at[0, 0 : n - 1])
    left(S_SHARE, srecv.at[0 : planes - 1])
    left(S_PAIR, spair)


def pass_on(*refs):
    count = len(refs) // 2
    stores = [
        pltpu.make_async_copy(refs[i], refs[count + i], refs[-1].at[i]) for i in range(count)
    ]
    for store in stores:
        store.start()
    for store in stores:
        store.wait()


def hand_over(arrays):
    count = len(arrays)
    return pl.pallas_call(
        pass_on,
        out_shape=tuple(jax.ShapeDtypeStruct(a.shape, a.dtype) for a in arrays),
        in_specs=[pl.BlockSpec(memory_space=pltpu.VMEM)] * count,
        out_specs=tuple([pl.BlockSpec(memory_space=pl.ANY)] * count),
        scratch_shapes=[pltpu.SemaphoreType.DMA((count,))],
    )(*(pltpu.with_memory_space_constraint(a, pltpu.VMEM) for a in arrays))


def fused_shards(
    tokens,
    cotangent,
    route_weights,
    routes,
    gate_proj,
    up_proj,
    down_proj,
    shared_down,
    shared_hidden,
):
    n = lax.axis_size("ep")
    tok_rows, feat = tokens.shape
    top = routes.shape[1]
    units = gate_proj.shape[2]
    hid = shared_hidden.shape[1]
    cap = 2 * tok_rows * top // n
    quarter = feat // 4
    planes = n // 2
    out_shape = (
        pltpu.VMEM((tok_rows, quarter), BF),
        pltpu.VMEM((top, tok_rows), F32),
        pltpu.VMEM((feat, units), BF),
        pltpu.VMEM((feat, units), BF),
        pltpu.VMEM((units, feat), BF),
        pltpu.VMEM((tok_rows, hid), BF),
        pltpu.VMEM((feat // n, hid), F32),
    )
    vmem = pl.BlockSpec(memory_space=pltpu.VMEM)
    hbm = pl.BlockSpec(memory_space=pl.ANY)
    per_piece = pltpu.VMEM((planes + 1, 8, 128), F32)
    outs = pl.pallas_call(
        functools.partial(kernel, n, cap),
        out_shape=out_shape,
        in_specs=[hbm] * 9,
        out_specs=(vmem,) * 7,
        scratch_shapes=[
            pltpu.VMEM((2, tok_rows, feat), BF),
            pltpu.VMEM((top, tok_rows), F32),
            pltpu.VMEM((top, tok_rows), jnp.int32),
            pltpu.VMEM((tok_rows, hid), BF),
            pltpu.VMEM((planes, 2, tok_rows, quarter), BF),
            pltpu.VMEM((planes, 8, tok_rows), F32),
            pltpu.VMEM((planes, 2 * cap, tok_rows), BF),
            pltpu.VMEM((n, cap, tok_rows), BF),
            pltpu.VMEM((planes + 1, 2, cap, quarter), BF),
            pltpu.VMEM((planes, 8, 2 * cap), F32),
            pltpu.VMEM((n, 8, 2 * cap), F32),
            pltpu.VMEM((planes, 4, 2, 2 * cap, quarter), BF),
            pltpu.VMEM((feat, 2 * units), BF),
            pltpu.VMEM((units, feat), BF),
            pltpu.VMEM((feat, hid), BF),
            pltpu.VMEM((planes, 2 * cap, units), BF),
            pltpu.VMEM((planes, 2 * cap, 2 * units), BF),
            pltpu.VMEM((planes, 2, 2, 2 * cap, quarter), BF),
            pltpu.VMEM((planes, 2, 2 * cap, quarter), BF),
            pltpu.VMEM((planes, 2 * cap, quarter), F32),
            pltpu.VMEM((planes, 2 * cap, quarter), BF),
            pltpu.VMEM((planes, 2 * cap, quarter), BF),
            pltpu.VMEM((planes, 2 * cap, quarter), BF),
            pltpu.VMEM((n, cap, quarter), BF),
            per_piece,
            per_piece,
            per_piece,
            per_piece,
            per_piece,
            pltpu.VMEM((n, 8, 128), F32),
            pltpu.VMEM((2, planes, feat // n, hid), BF),
            pltpu.VMEM((planes, feat // n, hid), BF),
            pltpu.VMEM((planes, feat // n, hid), BF),
            pltpu.VMEM((planes, feat // n, hid), BF),
            pltpu.SemaphoreType.DMA((SENDS,)),
            pltpu.SemaphoreType.DMA((ARRIVALS,)),
            pltpu.SemaphoreType.DMA((9,)),
        ],
        compiler_params=pltpu.CompilerParams(
            collective_id=0, has_side_effects=True, vmem_limit_bytes=48 * 1024 * 1024
        ),
    )(
        *(
            pltpu.with_memory_space_constraint(a, pltpu.HBM)
            for a in (
                tokens,
                cotangent,
                route_weights.T,
                routes.T,
                gate_proj[0],
                up_proj[0],
                down_proj[0],
                shared_down,
                shared_hidden,
            )
        )
    )
    outs = hand_over(outs)
    return outs[0], outs[1].T, outs[2][None], outs[3][None], outs[4][None], outs[5], outs[6]


def shards(*args):
    tokens, routes, gate_proj = args[0], args[3], args[4]
    n = lax.axis_size("ep")
    tok_rows, feat = tokens.shape
    top = routes.shape[1]
    fits = (
        gate_proj.shape[0] == 1
        and lax.axis_size("tp") == 4
        and n == 8
        and tok_rows == 128
        and 4 * tok_rows * top == n * tok_rows
        and 2 * top <= 8
        and feat % 512 == 0
        and feat // n % 128 == 0
    )
    if fits:
        return fused_shards(*args)
    return plain_shards(*args)


def plain_shards(
    tokens,
    cotangent,
    route_weights,
    routes,
    gate_proj,
    up_proj,
    down_proj,
    shared_down,
    shared_hidden,
):
    tok_rows, feat_width = tokens.shape
    top_count = routes.shape[1]
    exp_local = gate_proj.shape[0]
    ep_size = lax.axis_size("ep")
    tp_size = lax.axis_size("tp")
    exp_total = exp_local * ep_size
    capacity = 2 * tok_rows * top_count // exp_total
    quarter = feat_width // tp_size
    filled = exp_total * capacity
    flat_routes = routes.reshape(-1)
    one_hot = (flat_routes[:, None] == jnp.arange(exp_total, dtype=jnp.int32)[None, :]).astype(
        jnp.int32
    )
    rank_in = jnp.sum((jnp.cumsum(one_hot, axis=0) - one_hot) * one_hot, axis=1)
    slot_ids = flat_routes * capacity + rank_in
    route_owner = jnp.arange(flat_routes.shape[0], dtype=jnp.int32) // top_count
    owner_ids = jnp.full((filled,), tok_rows, jnp.int32).at[slot_ids].set(route_owner)
    sent_weights = (
        jnp.zeros((filled,), jnp.bfloat16)
        .at[slot_ids]
        .set(route_weights.reshape(-1).astype(jnp.bfloat16))
    )
    first_col = lax.axis_index("tp") * quarter
    own_rows = lax.dynamic_slice_in_dim(tokens, first_col, quarter, 1)
    own_grads = lax.dynamic_slice_in_dim(cotangent, first_col, quarter, 1)
    sent_rows = jnp.take(own_rows, owner_ids, axis=0, mode="fill", fill_value=0)
    sent_grads = jnp.take(own_grads, owner_ids, axis=0, mode="fill", fill_value=0)
    got_rows, got_grads, got_weights = (
        lax.all_to_all(sent_rows, "ep", split_axis=0, concat_axis=0, tiled=True),
        lax.all_to_all(sent_grads, "ep", split_axis=0, concat_axis=0, tiled=True),
        lax.all_to_all(sent_weights, "ep", split_axis=0, concat_axis=0, tiled=True),
    )
    got_rows, got_grads = (
        lax.all_gather(got_rows, "tp", axis=1, tiled=True),
        lax.all_gather(got_grads, "tp", axis=1, tiled=True),
    )
    slot_rows = got_rows.reshape(ep_size, exp_local, capacity, feat_width)
    slot_grads = got_grads.reshape(ep_size, exp_local, capacity, feat_width)
    weight_col = got_weights.reshape(ep_size, exp_local, capacity, 1).astype(jnp.float32)
    gate = jnp.einsum("secd,edf->secf", slot_rows, gate_proj, preferred_element_type=jnp.float32)
    upper = jnp.einsum("secd,edf->secf", slot_rows, up_proj, preferred_element_type=jnp.float32)
    active = jax.nn.silu(gate)
    hidden = (active * upper).astype(jnp.bfloat16)
    backed = jnp.einsum("secd,efd->secf", slot_grads, down_proj, preferred_element_type=jnp.float32)
    gate_share = jnp.sum(hidden.astype(jnp.float32) * backed, axis=3)
    d_hidden = weight_col * backed
    sigma = jax.nn.sigmoid(gate)
    d_gate = (d_hidden * upper * sigma * (1.0 + gate * (1.0 - sigma))).astype(jnp.bfloat16)
    d_up = (d_hidden * active).astype(jnp.bfloat16)
    scaled = (weight_col * slot_grads).astype(jnp.bfloat16)
    down_proj_grad = jnp.einsum(
        "secf,secd->efd", hidden, scaled, preferred_element_type=jnp.float32
    ).astype(jnp.bfloat16)
    gate_proj_grad = jnp.einsum(
        "secd,secf->edf", slot_rows, d_gate, preferred_element_type=jnp.float32
    ).astype(jnp.bfloat16)
    up_proj_grad = jnp.einsum(
        "secd,secf->edf", slot_rows, d_up, preferred_element_type=jnp.float32
    ).astype(jnp.bfloat16)
    partial_value = jnp.einsum(
        "secf,edf->secd", d_gate, gate_proj, preferred_element_type=jnp.float32
    )
    partial_value = partial_value + jnp.einsum(
        "secf,edf->secd", d_up, up_proj, preferred_element_type=jnp.float32
    )
    gate_whole = lax.psum(gate_share, "tp")
    input_cols = lax.psum_scatter(
        partial_value.astype(jnp.bfloat16), "tp", scatter_dimension=3, tiled=True
    )
    back_cols, back_gate = (
        lax.all_to_all(
            input_cols.reshape(filled, quarter), "ep", split_axis=0, concat_axis=0, tiled=True
        ),
        lax.all_to_all(
            gate_whole.astype(jnp.bfloat16).reshape(filled),
            "ep",
            split_axis=0,
            concat_axis=0,
            tiled=True,
        ),
    )
    picked = back_cols[slot_ids].reshape(tok_rows, top_count, quarter)
    tokens_grad = jnp.sum(picked.astype(jnp.float32), axis=1).astype(jnp.bfloat16)
    weights_grad = back_gate[slot_ids].astype(jnp.float32).reshape(tok_rows, top_count)
    hidden_grad = jnp.dot(cotangent, shared_down, preferred_element_type=jnp.float32).astype(
        jnp.bfloat16
    )
    shared_grad = lax.psum_scatter(
        jnp.einsum("td,th->dh", cotangent, shared_hidden, preferred_element_type=jnp.float32),
        "ep",
        scatter_dimension=0,
        tiled=True,
    )
    return (
        tokens_grad,
        weights_grad,
        gate_proj_grad,
        up_proj_grad,
        down_proj_grad,
        hidden_grad,
        shared_grad,
    )


def solution(mesh):
    in_specs = (
        P("ep", None),
        P("ep", None),
        P("ep", None),
        P("ep", None),
        P("ep", None, "tp"),
        P("ep", None, "tp"),
        P("ep", "tp", None),
        P(None, "tp"),
        P("ep", "tp"),
    )
    out_specs = (
        P("ep", "tp"),
        P("ep", None),
        P("ep", None, "tp"),
        P("ep", None, "tp"),
        P("ep", "tp", None),
        P("ep", "tp"),
        P("ep", "tp"),
    )
    return jax.shard_map(shards, mesh=mesh, in_specs=in_specs, out_specs=out_specs, check_vma=False)
```
